32 devices in a mesh: ep: 4 (over y, x), tp: 8 (over z, core).
Axes of the slice: x: 2, y: 2, z: 4, core: 2. Of those that a mesh axis runs over, the one named last changes fastest.
Arguments:
- tokens: bfloat16 [8192, 2048], P(('ep', 'tp')), may hold values from -6 to 6
- norm_gain: float32 [2048], replicated, may hold values from 0.1 to 1.9
- expert_ids: int32 [8192, 2], P(('ep', 'tp')), may hold values from 0 to 3, all different within a row; in each aligned block of 256 rows (0 to 255, 256 to 511, ...) at most 256 rows name the same one
- gate_weights: float32 [8192, 2], P(('ep', 'tp')), may hold values from 0.2 to 1
- w_gate: bfloat16 [4, 2048, 1024], P('ep', None, 'tp'), may hold values from -0.125 to 0.125
- w_up: bfloat16 [4, 2048, 1024], P('ep', None, 'tp'), may hold values from -0.125 to 0.125
- w_down: bfloat16 [4, 2048, 1024], P('ep', None, 'tp'), may hold values from -0.1875 to 0.1875
- dense_gate: bfloat16 [2048, 256], P('ep'), may hold values from -0.125 to 0.125
- dense_up: bfloat16 [2048, 256], P('ep'), may hold values from -0.125 to 0.125
- dense_down: bfloat16 [256, 2048], P(None, 'ep'), may hold values from -0.375 to 0.375
- mix_vector: float32 [2048], replicated, may hold values from -0.125 to 0.125
Outputs:
- mixed: bfloat16 [8192, 2048], P(('ep', 'tp'))
The draws below stay inside these ranges and needn't reach their ends.
Inputs may be any that keep to these rules, and one draw needn't show every extreme that they name: `expert_ids`: A row names 2 different experts. In the rows of one device (aligned blocks of 256 rows) each expert is named by at most 256 rows, a bound that some block reaches.
All inputs are finite; a program needn't handle non-finite values.
Results may differ from the reference program's by a relative error of at most 0.0075.
Values may be sent and summed in bfloat16 or wider, within the bound.
A program may use at most 320 MiB of HBM per device.

```python
import math
import jax
import jax.numpy as jnp
import numpy as np
from jax import lax

D = 2048
FF = 1024
FS = 256
TOPK = 2
TOK_DEV = 256
EXPERTS = 4
CAP = 256
TOKENS = 8192


def steps_of(own_key, shape, pieces, low, largest):
    def one(axis_at, parts):
        heights = jax.random.uniform(jax.random.fold_in(jax.random.fold_in(own_key, 6), axis_at), (parts,), jnp.float32, low / len(pieces), largest / len(pieces))
        return jnp.repeat(jnp.exp(heights), shape[axis_at] // parts).reshape((-1,) + (1,) * (len(shape) - axis_at - 1))

    level = one(*pieces[0])
    for cut in pieces[1:]:
        level = level * one(*cut)
    return level


def shared_out(stream_key, own, number, rows, amount, top, limit, slope):
    order = jax.random.permutation(stream_key, amount)
    crowded, ordinary = load_shares(amount, rows * top, limit, slope, True), load_shares(amount, rows * top, limit, slope, False)
    places = jnp.arange(amount)

    def named(tallies, turn):
        used = int((tallies > 0).sum())
        fixed = max(1, used // 4)
        passed = fixed + (places - fixed + turn * (used - fixed)) % max(1, amount - fixed)
        return jnp.zeros((amount,), jnp.int32).at[order[jnp.where(places < fixed, places, passed)]].set(jnp.asarray(tallies, jnp.int32))

    tallies = jnp.where(number % 4 == 0, named(crowded, number // 4), named(ordinary, number - number // 4 - 1))
    mixed = jax.random.permutation(jax.random.fold_in(own, 3), amount)
    source_of, sink = mixed[0:amount // 2 * 2:2], mixed[1:amount // 2 * 2:2]
    margin = jnp.minimum(tallies[source_of] - 1, limit - tallies[sink]) // 2
    margin = jnp.where((source_of == order[0]) | (sink == order[0]) | (tallies[sink] == 0), 0, jnp.maximum(margin, 0))
    passed = jax.random.randint(jax.random.fold_in(own, 4), (amount // 2,), 0, 1 << 20) % (margin + 1)
    tallies = tallies.at[source_of].add(-passed).at[sink].add(passed)
    labels = jnp.searchsorted(jnp.cumsum(tallies), jnp.arange(rows * top), side="right").astype(jnp.int32)
    table = labels.reshape(top, rows).T
    table = table[jax.random.permutation(jax.random.fold_in(own, 1), rows)]
    turn = jax.random.randint(jax.random.fold_in(own, 2), (rows, 1), 0, top)
    return jnp.take_along_axis(table, (jnp.arange(top)[None, :] + turn) % top, axis=1)


def load_shares(amount, total, bound, slope, full):
    portions = [(1 << 20) // math.isqrt(standing ** slope) + 1 for standing in range(1, amount + 1)]
    largest = bound if full else min(bound, max(-(-total // amount), total * portions[0] // sum(portions)))
    least = 1 if total - largest >= amount - 1 else 0
    counts, surplus = [largest] + [least] * (amount - 1), total - largest - least * (amount - 1)
    while surplus > 0:
        free = [i for i in range(1, amount) if counts[i] < largest] or [i for i in range(1, amount) if counts[i] < bound]
        pool, left = sum([portions[i] for i in free]), surplus
        for i in free:
            addition = min(bound - counts[i], max(1, left * portions[i] // pool), surplus)
            counts[i] = counts[i] + addition
            surplus = surplus - addition
    return np.array(counts)


def normal_values(rng, extent, spread, limit, pieces=(), held_as=jnp.bfloat16):
    values = spread * jax.random.normal(rng, extent, jnp.float32)
    if pieces:
        values = values * steps_of(rng, extent, pieces, -0.22, 0.18)
    return jnp.clip(values, -limit, limit).astype(held_as)


def setup_inputs(seed: int = 0) -> dict:
    keys = jax.random.split(jax.random.key(seed), 12)
    tokens = normal_values(keys[0], (TOKENS, D), 1.0, 6.0, ((0, 32),))
    norm_gain = jnp.clip(1.0 + 0.18 * jax.random.normal(keys[1], (D,), jnp.float32), 0.1, 1.9)
    expert_ids_keys = jax.random.split(jax.random.fold_in(keys[2], 1), TOKENS // TOK_DEV)
    expert_ids_turns = jax.random.permutation(jax.random.fold_in(keys[2], 3), TOKENS // TOK_DEV)
    expert_ids = jax.vmap(lambda own, number: shared_out(jax.random.fold_in(keys[2], 2), own, number, TOK_DEV, EXPERTS, TOPK, CAP, 2))(expert_ids_keys, expert_ids_turns).reshape((TOKENS, TOPK))
    gate_weights = jnp.clip(0.2 + 0.8 * jax.random.uniform(keys[3], (TOKENS, TOPK), jnp.float32) ** steps_of(keys[3], (TOKENS, TOPK), ((0, 32),), -0.2, 0.2), 0.2, 1.0)
    w_gate = normal_values(keys[4], (EXPERTS, D, FF), D ** -0.5, 0.125, ((0, 4), (2, 8)))
    w_up = normal_values(keys[5], (EXPERTS, D, FF), D ** -0.5, 0.125, ((0, 4), (2, 8)))
    w_down = normal_values(keys[6], (EXPERTS, D, FF), FF ** -0.5, 0.1875, ((0, 4), (2, 8)))
    dense_gate = normal_values(keys[7], (D, FS), D ** -0.5, 0.125, ((0, 4),))
    dense_up = normal_values(keys[8], (D, FS), D ** -0.5, 0.125, ((0, 4),))
    dense_down = normal_values(keys[9], (FS, D), FS ** -0.5, 0.375, ((1, 4),))
    mix_vector = normal_values(keys[10], (D,), D ** -0.5, 0.125, (), jnp.float32)
    return dict(tokens=tokens, norm_gain=norm_gain, expert_ids=expert_ids, gate_weights=gate_weights, w_gate=w_gate, w_up=w_up, w_down=w_down, dense_gate=dense_gate, dense_up=dense_up, dense_down=dense_down, mix_vector=mix_vector)


eps = 1e-06

def reference(tokens, norm_gain, expert_ids, gate_weights, w_gate, w_up, w_down, dense_gate, dense_up, dense_down, mix_vector):
    values = tokens.astype(jnp.float32)
    scale = lax.rsqrt(lax.optimization_barrier(jnp.mean(values * values, axis=1, keepdims=True)) + eps)
    normed = (values * scale * norm_gain).astype(jnp.bfloat16)
    blocks = TOKENS // TOK_DEV
    pairs = TOK_DEV * TOPK
    ids = expert_ids.reshape(blocks, pairs)
    onehot = (ids[:, :, None] == jnp.arange(EXPERTS, dtype=jnp.int32)[None, None, :]).astype(jnp.int32)
    before = jnp.cumsum(onehot, axis=1) - onehot
    slot = lax.optimization_barrier(jnp.sum(before * onehot, axis=2)).astype(jnp.int32)
    dest = (ids * CAP + slot).astype(jnp.int32)
    block_rows = jnp.arange(blocks, dtype=jnp.int32)[:, None]
    token_index = block_rows * TOK_DEV + (jnp.arange(pairs, dtype=jnp.int32) // TOPK)[None, :]
    table = jnp.full((blocks, EXPERTS * CAP), TOKENS, jnp.int32)
    table = table.at[block_rows, dest].set(token_index.astype(jnp.int32))
    weight_table = jnp.zeros((blocks, EXPERTS * CAP), jnp.float32)
    weight_table = weight_table.at[block_rows, dest].set(gate_weights.reshape(blocks, pairs))
    padded = jnp.concatenate([normed, jnp.zeros((1, D), jnp.bfloat16)], axis=0)

    def one_expert(total, expert):
        index = lax.dynamic_slice_in_dim(table, (expert * CAP).astype(jnp.int32), CAP, 1).reshape(-1)
        weight = lax.dynamic_slice_in_dim(weight_table, (expert * CAP).astype(jnp.int32), CAP, 1).reshape(-1)
        rows = padded[index]
        gate = jnp.dot(rows, w_gate[expert], preferred_element_type=jnp.float32)
        upper = jnp.dot(rows, w_up[expert], preferred_element_type=jnp.float32)
        hidden = (jax.nn.silu(gate) * upper).astype(jnp.bfloat16)
        result = jnp.dot(hidden, w_down[expert].T, preferred_element_type=jnp.float32).astype(jnp.bfloat16)
        return (total.at[index].add(weight[:, None] * result.astype(jnp.float32)), None)
    start = jnp.zeros((TOKENS + 1, D), jnp.float32)
    routed, unused = lax.scan(one_expert, start, jnp.arange(EXPERTS, dtype=jnp.int32))
    routed = routed[:TOKENS]
    dense_g = jnp.dot(normed, dense_gate, preferred_element_type=jnp.float32)
    dense_u = jnp.dot(normed, dense_up, preferred_element_type=jnp.float32)
    dense_hidden = (jax.nn.silu(dense_g) * dense_u).astype(jnp.bfloat16)
    dense_out = jnp.dot(dense_hidden, dense_down, preferred_element_type=jnp.float32)
    mix = jax.nn.sigmoid(lax.optimization_barrier(jnp.sum(normed.astype(jnp.float32) * mix_vector, axis=1)))
    return (routed + mix[:, None] * dense_out).astype(jnp.bfloat16)
```

```python
import functools

import jax
import jax.numpy as jnp
from jax import lax
from jax.experimental import pallas as pl
from jax.experimental.pallas import tpu as pltpu
from jax.sharding import PartitionSpec as P

MESH = pl.DeviceIdType.MESH
VMEM_BYTES = 65000 * 1024
CORES = 2
CHUNK = 256
SUB = 8
eps = 1e-06


def moe_kernel(
    ne, nz, x_hbm, wg_hbm, wu_hbm, wd_hbm, dg_hbm, du_hbm, dd_hbm, ids_ref, gates_ref,
    gain_ref, mixv_ref, out_ref,
    xin, xg, ws, wd, dgs, dus, dds, hbuf, own, keep, ysend, yrecv, relay, side, mix_ref, wts, wcol,
    lsem, wrecv, wright, wleft, wpartner, crecv, cright, cleft, cpartner,
    tsend, trecv, gsend, grecv, dsend, drecv, psend, precv, rsend, rrecv,
):
    me = lax.axis_index("ep")
    tp = lax.axis_index("tp")
    z = tp // CORES
    c = tp % CORES
    rows, width = xg.shape[1], xg.shape[2]
    nj, cw = ysend.shape[0], ysend.shape[3]
    half = rows // 2
    shard = ws.shape[4]
    across, along, diagonal = me + 1 - 2 * (me % 2), (me + 2) % ne, ne - 1 - me
    peers = [across, along, diagonal]
    partner = z * CORES + (1 - c)
    inner = (z > 0) & (z < nz - 1)

    local = [pltpu.make_async_copy(wg_hbm, ws.at[z, c, 0], lsem.at[0])]
    local.append(pltpu.make_async_copy(wu_hbm, ws.at[z, c, 1], lsem.at[1]))
    local.append(pltpu.make_async_copy(x_hbm, xin, lsem.at[2]))
    local.append(pltpu.make_async_copy(wd_hbm, wd.at[z, c], lsem.at[3]))
    for p, (ref, slot) in enumerate(((dg_hbm, dgs), (du_hbm, dus), (dd_hbm, dds))):
        local.append(pltpu.make_async_copy(ref, slot.at[me], lsem.at[4 + p]))
    for copy in local:
        copy.start()

    barrier = pltpu.get_barrier_semaphore()
    for peer in peers:
        pl.semaphore_signal(barrier, inc=1, device_id={"ep": peer}, device_id_type=MESH)
    pl.semaphore_signal(barrier, inc=1, device_id={"tp": partner}, device_id_type=MESH)

    @pl.when(z > 0)
    def _():
        pl.semaphore_signal(barrier, inc=1, device_id={"tp": tp - CORES}, device_id_type=MESH)

    @pl.when(z < nz - 1)
    def _():
        pl.semaphore_signal(barrier, inc=1, device_id={"tp": tp + CORES}, device_id_type=MESH)

    neighbours = (z + nz - 1) // nz + (2 * nz - 2 - z) // nz
    pl.semaphore_wait(barrier, ne + neighbours)

    def remote(src, dst, send, recv, **device):
        return pltpu.make_async_remote_copy(
            src_ref=src, dst_ref=dst, send_sem=send, recv_sem=recv,
            device_id=device, device_id_type=MESH,
        )

    def weight_copy(src, p, target, sems):
        piece = ws.at[src, c, p]
        return remote(piece, piece, sems.at[src, p], wrecv.at[src, c, p], tp=target)

    def to_right(src, p):
        return weight_copy(src, p, tp + CORES, wright)

    def to_left(src, p):
        return weight_copy(src, p, tp - CORES, wleft)

    def to_partner(src, p):
        return weight_copy(src, p, partner, wpartner)

    def await_piece(src, color, p):
        piece = ws.at[src, color, p]
        remote(piece, piece, wpartner.at[src, p], wrecv.at[src, color, p], tp=partner).wait_recv()

    def chunk(j):
        return pl.ds(pl.multiple_of(j * cw, cw), cw)

    def chunk_copy(src, j, target, sems):
        piece = wd.at[src, c, chunk(j)]
        return remote(piece, piece, sems.at[src], crecv.at[j, src, c], tp=target)

    def c_right(src, j):
        chunk_copy(src, j, tp + CORES, cright).start()

    def c_left(src, j):
        chunk_copy(src, j, tp - CORES, cleft).start()

    def c_partner(src, j):
        chunk_copy(src, j, partner, cpartner).start()

    def await_chunk(src, color, j):
        piece = wd.at[src, color, chunk(j)]
        remote(piece, piece, cpartner.at[src], crecv.at[j, src, color], tp=partner).wait_recv()

    def await_sent(src, sems):
        piece = wd.at[src, c]
        remote(piece, piece, sems.at[src], crecv.at[0, src, c], tp=partner).wait_send()

    def token_copy(k):
        block = (me, me, across, along)[k]
        peer = (across, along, along, across)[k]
        low, size = ((0, rows), (0, rows), (0, half), (half, half))[k]
        piece = xg.at[block, low : low + size]
        return remote(piece, piece, tsend.at[k], trecv.at[k], ep=peer)

    def await_token(k):
        block = (across, along, diagonal, diagonal)[k]
        low, size = ((0, rows), (0, rows), (0, half), (half, half))[k]
        piece = xg.at[block, low : low + size]
        remote(piece, piece, tsend.at[k], trecv.at[k], ep=across).wait_recv()

    def gate_copy(k, block):
        return remote(wts.at[block], wts.at[block], gsend.at[k], grecv.at[block], ep=peers[k])

    def dense_piece(p, block, color):
        slot = (dgs, dus, dds)[p]
        part = slot.shape[1] // CORES
        return slot.at[block, pl.ds(pl.multiple_of(color * part, part), part)]

    def dense_copy(k, p, block):
        piece = dense_piece(p, block, c)
        return remote(piece, piece, dsend.at[k, p], drecv.at[block, p], ep=peers[k])

    def dense_partner(k, p, color):
        piece = dense_piece(p, peers[k], color)
        return remote(piece, piece, psend.at[k, p], precv.at[k, p], tp=partner)

    for p in range(2):
        local[p].wait()

        @pl.when(z < nz - 1)
        def _():
            to_right(z, p).start()

        @pl.when(z > 0)
        def _():
            to_left(z, p).start()

        to_partner(z, p).start()
    local[2].wait()

    expert = lax.broadcasted_iota(jnp.int32, (SUB, rows), 0)
    named, gate = ids_ref[...], gates_ref[...]
    weight = jnp.zeros((SUB, rows), jnp.float32)
    for k in range(ids_ref.shape[0]):
        weight += jnp.where(named[k : k + 1, :] == expert, gate[k : k + 1, :], 0.0)
    wts[me] = weight
    tile = 32

    def norm(i, carry):
        at = pl.ds(pl.multiple_of(i * tile, tile), tile)
        v = xin[at, :].astype(jnp.float32)
        scale = lax.rsqrt(jnp.sum(v * v, axis=1, keepdims=True) * (1.0 / width) + eps)
        n = (v * scale * gain_ref[...]).astype(jnp.bfloat16)
        xg[me, at, :] = n
        m = jnp.sum(n.astype(jnp.float32) * mixv_ref[...], axis=1, keepdims=True)
        mix_ref[at, :] = 1.0 / (1.0 + jnp.exp(-m))
        return carry

    lax.fori_loop(0, rows // tile, norm, 0)
    local[3].wait()

    def own_chunks(j, carry):
        c_partner(z, j)

        @pl.when(z == 0)
        def _():
            c_right(z, j)

        @pl.when(z == nz - 1)
        def _():
            c_left(z, j)

        return carry

    lax.fori_loop(0, nj, own_chunks, 0)
    for k in range(2):
        token_copy(k).start()
    for k in range(ne - 1):
        gate_copy(k, me).start()
    for p in range(3):
        local[4 + p].wait()
    for p in range(3):
        for k in range(ne - 1):
            dense_copy(k, p, me).start()

    def forward(d, p):
        @pl.when(z >= d)
        def _():
            await_piece(z - d, c, p)

            @pl.when(z < nz - 1)
            def _():
                to_right(z - d, p).start()

            to_partner(z - d, p).start()

        @pl.when(z + d < nz)
        def _():
            await_piece(z + d, c, p)

            @pl.when(z > 0)
            def _():
                to_left(z + d, p).start()

            to_partner(z + d, p).start()

    def hidden(src):
        await_piece(src, 1 - c, 0)
        await_piece(src, 1 - c, 1)
        at = pl.ds(pl.multiple_of(src * (CORES * shard), CORES * shard), CORES * shard)

        def one(b, carry):
            x = xg[b]
            wg = jnp.concatenate([ws[src, i, 0] for i in range(CORES)], axis=1)
            g = jnp.dot(x, wg, preferred_element_type=jnp.float32)
            wu = jnp.concatenate([ws[src, i, 1] for i in range(CORES)], axis=1)
            u = jnp.dot(x, wu, preferred_element_type=jnp.float32)
            hbuf[b, :, at] = (g / (1.0 + jnp.exp(-g)) * u * wcol[b]).astype(jnp.bfloat16)
            return carry

        lax.fori_loop(0, ne, one, 0)

    def both(d, fn):
        @pl.when(z >= d)
        def _():
            fn(z - d)

        @pl.when(z + d < nz)
        def _():
            fn(z + d)

    def own_chunk(j):
        @pl.when(inner)
        def _():
            c_right(z, j)
            c_left(z, j)

    for p in range(2):
        forward(1, p)
    for k in range(2):
        await_token(k)
        token_copy(2 + k).start()
    for d in range(2, nz - 1):
        for p in range(2):
            forward(d, p)
    for j in range(2):
        own_chunk(j)
    for k in range(ne - 1):
        gate_copy(k, peers[k]).wait_recv()
    lane = lax.broadcasted_iota(jnp.int32, (rows, SUB), 1)
    for b in range(ne):
        column = jnp.where(lane == me, wts[b].T, 0.0)
        wcol[b] = jnp.sum(column, axis=1, keepdims=True)
    for k in range(2, 4):
        await_token(k)
    hidden(z)
    for d in range(1, nz - 1):
        both(d, hidden)
    for k in range(ne - 1):
        for p in range(3):
            dense_copy(k, p, peers[k]).wait_recv()
            dense_partner(k, p, c).start()
    forward(nz - 1, 0)
    for k in range(ne - 1):
        for p in range(3):
            dense_partner(k, p, 1 - c).wait_recv()
    dense_side(ne, me, xg, dgs, dus, dds, mix_ref, side)
    forward(nz - 1, 1)
    both(nz - 1, hidden)

    def back(k, j):
        block = (diagonal, diagonal, across, along, along, across)[k]
        peer = (across, along, across, along, along, across)[k]
        low = (0, half, 0, half, 0, half)[k]
        spot = (0, 1, 0, 1, 1, 0)[k]
        lands = relay.at[j, k] if k < 2 else yrecv.at[j, spot, low : low + half]
        return remote(
            ysend.at[j, block, low : low + half], lands, rsend.at[k], rrecv.at[j, k], ep=peer
        )

    def await_back(k):
        piece = relay.at[:, 0]
        remote(piece, piece, rsend.at[k], rrecv.at[0, k], ep=across).wait_send()

    def take(j):
        @pl.when(j + 2 < nj)
        def _():
            own_chunk(j + 2)

        for d in range(1, nz):
            @pl.when(z >= d)
            def _():
                await_chunk(z - d, c, j)

                @pl.when(z < nz - 1)
                def _():
                    c_right(z - d, j)

                c_partner(z - d, j)

            @pl.when(z + d < nz)
            def _():
                await_chunk(z + d, c, j)

                @pl.when(z > 0)
                def _():
                    c_left(z + d, j)

                c_partner(z + d, j)

        for src in range(nz):
            await_chunk(src, 1 - c, j)

    def produce(j):
        at = chunk(j)
        w = jnp.concatenate([wd[s, i, at, :] for s in range(nz) for i in range(CORES)], axis=1)

        def rows_of(b):
            return lax.dot_general(
                hbuf[b], w, (((1,), (1,)), ((), ())), preferred_element_type=jnp.float32
            )

        ysend[j, diagonal] = rows_of(diagonal).astype(jnp.bfloat16)
        back(0, j).start()
        back(1, j).start()
        y = rows_of(across)
        ysend[j, across, :half] = y[:half].astype(jnp.bfloat16)
        keep[j, 1] = y[half:]
        back(2, j).start()
        y = rows_of(along)
        ysend[j, along, half:] = y[half:].astype(jnp.bfloat16)
        keep[j, 0] = y[:half]
        back(3, j).start()
        own[:, at] = rows_of(me)

    def pass_on(j):
        back(0, j).wait_recv()
        v = keep[j, 0] + relay[j, 0].astype(jnp.float32)
        ysend[j, along, :half] = v.astype(jnp.bfloat16)
        back(4, j).start()
        back(1, j).wait_recv()
        v = keep[j, 1] + relay[j, 1].astype(jnp.float32)
        ysend[j, across, half:] = v.astype(jnp.bfloat16)
        back(5, j).start()

    def combine(j):
        for k in range(2, 6):
            back(k, j).wait_recv()
        at = chunk(j)
        total = side[:, at] + own[:, at]
        for k in range(2):
            total = total + yrecv[j, k].astype(jnp.float32)
        out_ref[:, at] = total.astype(jnp.bfloat16)

    def step(j, carry):
        take(j)
        produce(j)

        @pl.when(j >= 1)
        def _():
            pass_on(j - 1)

        @pl.when(j >= 2)
        def _():
            combine(j - 2)

        return carry

    lax.fori_loop(0, nj, step, 0)
    pass_on(nj - 1)
    combine(nj - 2)
    combine(nj - 1)

    for k in range(4):
        token_copy(k).wait_send()
    for k in range(ne - 1):
        gate_copy(k, me).wait_send()
        for p in range(3):
            dense_copy(k, p, me).wait_send()
            dense_partner(k, p, c).wait_send()
    for src in range(nz):
        @pl.when((z < nz - 1) & (z >= src))
        def _():
            for p in range(2):
                to_right(src, p).wait_send()
            await_sent(src, cright)

        @pl.when((z > 0) & (z <= src))
        def _():
            for p in range(2):
                to_left(src, p).wait_send()
            await_sent(src, cleft)

        for p in range(2):
            to_partner(src, p).wait_send()
        await_sent(src, cpartner)
    for k in range(6):
        await_back(k)


def dense_side(ne, me, xg, dgs, dus, dds, mix_ref, side):
    deep, wide = dgs.shape[1], dds.shape[2]
    g = u = None
    for e in range(ne):
        x = xg[me, :, e * deep : (e + 1) * deep]
        ge = jnp.dot(x, dgs[e], preferred_element_type=jnp.float32)
        ue = jnp.dot(x, dus[e], preferred_element_type=jnp.float32)
        g, u = (ge, ue) if e == 0 else (g + ge, u + ue)
    h = (g / (1.0 + jnp.exp(-g)) * u).astype(jnp.bfloat16)
    for e in range(ne):
        o = jnp.dot(h, dds[e], preferred_element_type=jnp.float32)
        side[:, e * wide : (e + 1) * wide] = mix_ref[...] * o


def fused_layer(
    ne, tp, tokens, norm_gain, expert_ids, gate_weights,
    w_gate, w_up, w_down, dense_gate, dense_up, dense_down, mix_vector,
):
    nz = tp // CORES
    rows, width = tokens.shape
    shard = w_gate.shape[2]
    nj = width // CHUNK
    half = rows // 2
    bf, f32 = jnp.bfloat16, jnp.float32
    dma = pltpu.SemaphoreType.DMA
    hbm = pl.BlockSpec(memory_space=pl.ANY)
    vmem = pl.BlockSpec(memory_space=pltpu.VMEM)
    flops = 6 * ne * rows * width * shard * tp
    return pl.pallas_call(
        functools.partial(moe_kernel, ne, nz),
        out_shape=jax.ShapeDtypeStruct((rows, width), bf),
        in_specs=[hbm] * 7 + [vmem] * 4,
        out_specs=vmem,
        scratch_shapes=[
            pltpu.VMEM((rows, width), bf),
            pltpu.VMEM((ne, rows, width), bf),
            pltpu.VMEM((nz, CORES, 2, width, shard), bf),
            pltpu.VMEM((nz, CORES, width, shard), bf),
            pltpu.VMEM((ne,) + dense_gate.shape, bf),
            pltpu.VMEM((ne,) + dense_up.shape, bf),
            pltpu.VMEM((ne,) + dense_down.shape, bf),
            pltpu.VMEM((ne, rows, tp * shard), bf),
            pltpu.VMEM((rows, width), f32),
            pltpu.VMEM((nj, 2, half, CHUNK), f32),
            pltpu.VMEM((nj, ne, rows, CHUNK), bf),
            pltpu.VMEM((nj, 2, rows, CHUNK), bf),
            pltpu.VMEM((nj, 2, half, CHUNK), bf),
            pltpu.VMEM((rows, width), f32),
            pltpu.VMEM((rows, 1), f32),
            pltpu.VMEM((ne, SUB, rows), f32),
            pltpu.VMEM((ne, rows, 1), f32),
            dma((7,)),
            dma((nz, CORES, 2)),
            dma((nz, 2)),
            dma((nz, 2)),
            dma((nz, 2)),
            dma((nj, nz, CORES)),
            dma((nz,)),
            dma((nz,)),
            dma((nz,)),
            dma((4,)),
            dma((4,)),
            dma((ne,)),
            dma((ne,)),
            dma((ne, 3)),
            dma((ne, 3)),
            dma((ne, 3)),
            dma((ne, 3)),
            dma((6,)),
            dma((nj, 6)),
        ],
        compiler_params=pltpu.CompilerParams(
            collective_id=0, has_side_effects=True, vmem_limit_bytes=VMEM_BYTES
        ),
        cost_estimate=pl.CostEstimate(
            flops=flops, bytes_accessed=8 * rows * width, transcendentals=ne * rows * shard * tp
        ),
    )(
        tokens, w_gate[0], w_up[0], w_down[0], dense_gate, dense_up, dense_down,
        expert_ids.T, gate_weights.T, norm_gain.reshape(1, width), mix_vector.reshape(1, width),
    )


def fits(ne, tp, tokens, w_gate, dense_gate):
    rows, width = tokens.shape
    shard = w_gate.shape[2]
    block = rows * width
    size = 2 * ne * block * 2 + 24 * block + 6 * width * shard * tp
    size += 2 * ne * rows * shard * tp + 6 * ne * dense_gate.size + 1024 * ne * rows
    aligned = shard % 128 == 0 and width % (2 * CHUNK) == 0 and rows % 64 == 0
    return ne == 4 and tp % CORES == 0 and tp > 2 * CORES and aligned and size < VMEM_BYTES * 15 // 16


def dense_branch(normed, dense_gate, dense_up, dense_down, mix_vector):
    dense_g = jnp.dot(
        normed,
        lax.all_gather(dense_gate, "ep", axis=0, tiled=True),
        preferred_element_type=jnp.float32,
    )
    dense_u = jnp.dot(
        normed,
        lax.all_gather(dense_up, "ep", axis=0, tiled=True),
        preferred_element_type=jnp.float32,
    )
    dense_hidden = (jax.nn.silu(dense_g) * dense_u).astype(jnp.bfloat16)
    dense_out = jnp.dot(
        dense_hidden,
        lax.all_gather(dense_down, "ep", axis=1, tiled=True),
        preferred_element_type=jnp.float32,
    )
    mix = jax.nn.sigmoid(jnp.sum(normed.astype(jnp.float32) * mix_vector, axis=1))
    return mix[:, None] * dense_out


def on_device(
    tokens,
    norm_gain,
    expert_ids,
    gate_weights,
    w_gate,
    w_up,
    w_down,
    dense_gate,
    dense_up,
    dense_down,
    mix_vector,
):
    groups = lax.axis_size("ep")
    ring = lax.axis_size("tp")
    if fits(groups, ring, tokens, w_gate, dense_gate):
        return fused_layer(
            groups, ring, tokens, norm_gain, expert_ids, gate_weights,
            w_gate, w_up, w_down, dense_gate, dense_up, dense_down, mix_vector,
        )
    values = tokens.astype(jnp.float32)
    scale = lax.rsqrt(jnp.mean(values * values, axis=1, keepdims=True) + eps)
    normed = (values * scale * norm_gain).astype(jnp.bfloat16)
    count_tok, topk = expert_ids.shape
    width = tokens.shape[1]
    capacity = 2 * count_tok * topk // groups
    flat_ids = expert_ids.reshape(-1)
    onehot = (flat_ids[:, None] == jnp.arange(groups, dtype=jnp.int32)[None, :]).astype(jnp.int32)
    before = jnp.cumsum(onehot, axis=0) - onehot
    slot = jnp.sum(before * onehot, axis=1)
    dest = flat_ids * capacity + slot
    owner = jnp.arange(count_tok * topk, dtype=jnp.int32) // topk
    buffer = jnp.zeros((groups * capacity, width), jnp.bfloat16).at[dest].set(normed[owner])
    arrived = lax.all_to_all(
        buffer.reshape(groups, capacity, width), "ep", split_axis=0, concat_axis=0, tiled=True
    )
    rows = arrived.reshape(groups * capacity, width)
    gate = jnp.dot(
        rows,
        lax.all_gather(w_gate, "tp", axis=2, tiled=True)[0],
        preferred_element_type=jnp.float32,
    )
    upper = jnp.dot(
        rows, lax.all_gather(w_up, "tp", axis=2, tiled=True)[0], preferred_element_type=jnp.float32
    )
    hidden_all = (jax.nn.silu(gate) * upper).astype(jnp.bfloat16)
    expert_out = lax.dot_general(
        hidden_all,
        lax.all_gather(w_down, "tp", axis=2, tiled=True)[0],
        (((1,), (1,)), ((), ())),
        preferred_element_type=jnp.float32,
    )
    results = expert_out.astype(jnp.bfloat16).reshape(groups, capacity, width)
    returned = lax.all_to_all(results, "ep", split_axis=0, concat_axis=0, tiled=True)
    picked = returned.reshape(groups * capacity, width)[dest].reshape(count_tok, topk, width)
    routed = jnp.einsum("tk,tkd->td", gate_weights, picked.astype(jnp.float32))
    side = dense_branch(normed, dense_gate, dense_up, dense_down, mix_vector)
    return (routed + side).astype(jnp.bfloat16)


def solution(mesh):
    placed = (
        P(("ep", "tp"), None),
        P(),
        P(("ep", "tp"), None),
        P(("ep", "tp"), None),
        P("ep", None, "tp"),
        P("ep", None, "tp"),
        P("ep", None, "tp"),
        P("ep", None),
        P("ep", None),
        P(None, "ep"),
        P(),
    )
    return jax.shard_map(
        on_device, mesh=mesh, in_specs=placed, out_specs=P(("ep", "tp"), None), check_vma=False
    )
```

```python
import functools

import jax
import jax.numpy as jnp
from jax import lax
from jax.experimental import pallas as pl
from jax.experimental.pallas import tpu as pltpu
from jax.sharding import PartitionSpec as P

MESH = pl.DeviceIdType.MESH
VMEM_BYTES = 64000 * 1024
CORES = 2
CHUNK = 256
SUB = 8
eps = 1e-06


def moe_kernel(
    ne, nz, x_hbm, wg_hbm, wu_hbm, wd_hbm, dg_hbm, du_hbm, dd_hbm, ids_ref, gates_ref,
    gain_ref, mixv_ref, out_ref,
    xin, xg, ws, wd, dgs, dus, dds, hbuf, own, keep, ysend, yrecv, relay, side, mix_ref, wts, wcol,
    lsem, wrecv, wright, wleft, wpartner, crecv, cright, cleft, cpartner,
    tsend, trecv, gsend, grecv, dsend, drecv, psend, precv, rsend, rrecv,
):
    me = lax.axis_index("ep")
    tp = lax.axis_index("tp")
    z = tp // CORES
    c = tp % CORES
    rows, width = xg.shape[1], xg.shape[2]
    nj, cw = ysend.shape[0], ysend.shape[3]
    half = rows // 2
    shard = ws.shape[4]
    across, along, diagonal = me + 1 - 2 * (me % 2), (me + 2) % ne, ne - 1 - me
    peers = [across, along, diagonal]
    partner = z * CORES + (1 - c)

    local = [pltpu.make_async_copy(wg_hbm, ws.at[z, c, 0], lsem.at[0])]
    local.append(pltpu.make_async_copy(wu_hbm, ws.at[z, c, 1], lsem.at[1]))
    local.append(pltpu.make_async_copy(x_hbm, xin, lsem.at[2]))
    local.append(pltpu.make_async_copy(wd_hbm, wd.at[z, c], lsem.at[3]))
    for p, (ref, slot) in enumerate(((dg_hbm, dgs), (du_hbm, dus), (dd_hbm, dds))):
        local.append(pltpu.make_async_copy(ref, slot.at[me], lsem.at[4 + p]))
    for copy in local:
        copy.start()

    barrier = pltpu.get_barrier_semaphore()
    for peer in peers:
        pl.semaphore_signal(barrier, inc=1, device_id={"ep": peer}, device_id_type=MESH)
    pl.semaphore_signal(barrier, inc=1, device_id={"tp": partner}, device_id_type=MESH)

    @pl.when(z > 0)
    def _():
        pl.semaphore_signal(barrier, inc=1, device_id={"tp": tp - CORES}, device_id_type=MESH)

    @pl.when(z < nz - 1)
    def _():
        pl.semaphore_signal(barrier, inc=1, device_id={"tp": tp + CORES}, device_id_type=MESH)

    neighbours = (z + nz - 1) // nz + (2 * nz - 2 - z) // nz
    with jax.named_scope("barrier"):
        pl.semaphore_wait(barrier, ne + neighbours)

    def remote(src, dst, send, recv, **device):
        return pltpu.make_async_remote_copy(
            src_ref=src, dst_ref=dst, send_sem=send, recv_sem=recv,
            device_id=device, device_id_type=MESH,
        )

    def weight_copy(src, p, target, sems):
        piece = ws.at[src, c, p]
        return remote(piece, piece, sems.at[src, p], wrecv.at[src, c, p], tp=target)

    def to_right(src, p):
        return weight_copy(src, p, tp + CORES, wright)

    def to_left(src, p):
        return weight_copy(src, p, tp - CORES, wleft)

    def to_partner(src, p):
        return weight_copy(src, p, partner, wpartner)

    def await_piece(src, color, p):
        piece = ws.at[src, color, p]
        remote(piece, piece, wpartner.at[src, p], wrecv.at[src, color, p], tp=partner).wait_recv()

    def chunk(j):
        return pl.ds(pl.multiple_of(j * cw, cw), cw)

    def chunk_copy(src, j, target, sems):
        piece = wd.at[src, c, chunk(j)]
        return remote(piece, piece, sems.at[src], crecv.at[j, src, c], tp=target)

    def c_right(src, j):
        chunk_copy(src, j, tp + CORES, cright).start()

    def c_left(src, j):
        chunk_copy(src, j, tp - CORES, cleft).start()

    def c_partner(src, j):
        chunk_copy(src, j, partner, cpartner).start()

    def await_chunk(src, color, j):
        piece = wd.at[src, color, chunk(j)]
        remote(piece, piece, cpartner.at[src], crecv.at[j, src, color], tp=partner).wait_recv()

    def await_sent(src, sems):
        piece = wd.at[src, c]
        remote(piece, piece, sems.at[src], crecv.at[0, src, c], tp=partner).wait_send()

    def token_copy(k):
        block = (me, me, across, along)[k]
        peer = (across, along, along, across)[k]
        low, size = ((0, rows), (0, rows), (0, half), (half, half))[k]
        piece = xg.at[block, low : low + size]
        return remote(piece, piece, tsend.at[k], trecv.at[k], ep=peer)

    def await_token(k):
        block = (across, along, diagonal, diagonal)[k]
        low, size = ((0, rows), (0, rows), (0, half), (half, half))[k]
        piece = xg.at[block, low : low + size]
        remote(piece, piece, tsend.at[k], trecv.at[k], ep=across).wait_recv()

    def gate_copy(k, block):
        return remote(wts.at[block], wts.at[block], gsend.at[k], grecv.at[block], ep=peers[k])

    def dense_piece(p, block, color):
        slot = (dgs, dus, dds)[p]
        part = slot.shape[1] // CORES
        return slot.at[block, pl.ds(pl.multiple_of(color * part, part), part)]

    def dense_copy(k, p, block):
        piece = dense_piece(p, block, c)
        return remote(piece, piece, dsend.at[k, p], drecv.at[block, p], ep=peers[k])

    def dense_partner(k, p, color):
        piece = dense_piece(p, peers[k], color)
        return remote(piece, piece, psend.at[k, p], precv.at[k, p], tp=partner)

    for p in range(2):
        local[p].wait()

        @pl.when(z < nz - 1)
        def _():
            to_right(z, p).start()

        @pl.when(z > 0)
        def _():
            to_left(z, p).start()

        to_partner(z, p).start()
    local[2].wait()

    expert = lax.broadcasted_iota(jnp.int32, (SUB, rows), 0)
    named, gate = ids_ref[...], gates_ref[...]
    weight = jnp.zeros((SUB, rows), jnp.float32)
    for k in range(ids_ref.shape[0]):
        weight += jnp.where(named[k : k + 1, :] == expert, gate[k : k + 1, :], 0.0)
    wts[me] = weight
    tile = 32

    def norm(i, carry):
        at = pl.ds(pl.multiple_of(i * tile, tile), tile)
        v = xin[at, :].astype(jnp.float32)
        scale = lax.rsqrt(jnp.sum(v * v, axis=1, keepdims=True) * (1.0 / width) + eps)
        n = (v * scale * gain_ref[...]).astype(jnp.bfloat16)
        xg[me, at, :] = n
        m = jnp.sum(n.astype(jnp.float32) * mixv_ref[...], axis=1, keepdims=True)
        mix_ref[at, :] = 1.0 / (1.0 + jnp.exp(-m))
        return carry

    with jax.named_scope("norm"):
        lax.fori_loop(0, rows // tile, norm, 0)
    local[3].wait()

    def own_chunks(j, carry):
        c_partner(z, j)

        @pl.when(z == 0)
        def _():
            c_right(z, j)

        @pl.when(z == nz - 1)
        def _():
            c_left(z, j)

        return carry

    lax.fori_loop(0, nj, own_chunks, 0)
    for k in range(2):
        token_copy(k).start()
    for k in range(ne - 1):
        gate_copy(k, me).start()

    def forward(d, p):
        @pl.when(z >= d)
        def _():
            await_piece(z - d, c, p)

            @pl.when(z < nz - 1)
            def _():
                to_right(z - d, p).start()

            to_partner(z - d, p).start()

        @pl.when(z + d < nz)
        def _():
            await_piece(z + d, c, p)

            @pl.when(z > 0)
            def _():
                to_left(z + d, p).start()

            to_partner(z + d, p).start()

    def hidden(src):
        await_piece(src, 1 - c, 0)
        await_piece(src, 1 - c, 1)
        at = pl.ds(pl.multiple_of(src * (CORES * shard), CORES * shard), CORES * shard)

        def one(b, carry):
            x = xg[b]
            wg = jnp.concatenate([ws[src, i, 0] for i in range(CORES)], axis=1)
            g = jnp.dot(x, wg, preferred_element_type=jnp.float32)
            wu = jnp.concatenate([ws[src, i, 1] for i in range(CORES)], axis=1)
            u = jnp.dot(x, wu, preferred_element_type=jnp.float32)
            hbuf[b, :, at] = (g / (1.0 + jnp.exp(-g)) * u * wcol[b]).astype(jnp.bfloat16)
            return carry

        lax.fori_loop(0, ne, one, 0)

    def both(d, fn):
        @pl.when(z >= d)
        def _():
            fn(z - d)

        @pl.when(z + d < nz)
        def _():
            fn(z + d)

    def arrive(src, j):
        await_chunk(src, c, j)
        c_partner(src, j)

    def ahead(t):
        for d in range(nz - 1):
            j = t + nz - 1 - d

            @pl.when((z == 1) & (j >= 0) & (j < nj))
            def _():
                if d == 0:
                    c_right(z, j)
                elif d == 1:
                    arrive(z - 1, j)
                    c_right(z - 1, j)
                    arrive(z + 1, j)
                else:
                    arrive(z + 2, j)
                    for src in range(nz - 1):
                        c_left(z + src, j)

            @pl.when((z == 2) & (j >= 0) & (j < nj))
            def _():
                if d == 0:
                    c_left(z, j)
                elif d == 1:
                    arrive(z + 1, j)
                    c_left(z + 1, j)
                    arrive(z - 1, j)
                else:
                    arrive(z - 2, j)
                    for src in range(nz - 1):
                        c_right(z - src, j)

    for p in range(2):
        with jax.named_scope(f"forward1_{p}"):
            forward(1, p)
    with jax.named_scope("token_relay"):
        for k in range(2):
            await_token(k)
            token_copy(2 + k).start()
    for p in range(3):
        local[4 + p].wait()
        for k in range(ne - 1):
            dense_copy(k, p, me).start()
    for d in range(2, nz - 1):
        for p in range(2):
            with jax.named_scope(f"forward{d}_{p}"):
                forward(d, p)
    ahead(1 - nz)
    with jax.named_scope("gate_wait"):
        for k in range(ne - 1):
            gate_copy(k, peers[k]).wait_recv()
    lane = lax.broadcasted_iota(jnp.int32, (rows, SUB), 1)
    for b in range(ne):
        column = jnp.where(lane == me, wts[b].T, 0.0)
        wcol[b] = jnp.sum(column, axis=1, keepdims=True)
    with jax.named_scope("token_wait"):
        for k in range(2, 4):
            await_token(k)
    with jax.named_scope("hidden_own"):
        hidden(z)
    for d in range(1, nz - 1):
        with jax.named_scope(f"ahead{d}"):
            ahead(d + 1 - nz)
        with jax.named_scope(f"hidden{d}"):
            both(d, hidden)
    with jax.named_scope("dense_wait"):
        for k in range(ne - 1):
            for p in range(3):
                dense_copy(k, p, peers[k]).wait_recv()
                dense_partner(k, p, c).start()
    with jax.named_scope("forward_last0"):
        forward(nz - 1, 0)
    with jax.named_scope("dense_partner"):
        for k in range(ne - 1):
            for p in range(3):
                dense_partner(k, p, 1 - c).wait_recv()
    with jax.named_scope("dense_side"):
        dense_side(ne, me, xg, dgs, dus, dds, mix_ref, side)
    with jax.named_scope("forward_last1"):
        forward(nz - 1, 1)
    with jax.named_scope("hidden_last"):
        both(nz - 1, hidden)

    def back(k, j):
        block = (diagonal, diagonal, across, along, along, across)[k]
        peer = (across, along, across, along, along, across)[k]
        low = (0, half, 0, half, 0, half)[k]
        spot = (0, 1, 0, 1, 1, 0)[k]
        lands = relay.at[j, k] if k < 2 else yrecv.at[j, spot, low : low + half]
        return remote(
            ysend.at[j, block, low : low + half], lands, rsend.at[k], rrecv.at[j, k], ep=peer
        )

    def await_back(k):
        piece = relay.at[:, 0]
        remote(piece, piece, rsend.at[k], rrecv.at[0, k], ep=across).wait_send()

    def take(j):
        ahead(j)

        @pl.when(z == 0)
        def _():
            for d in range(1, nz):
                arrive(d, j)

        @pl.when(z == nz - 1)
        def _():
            for d in range(1, nz):
                arrive(z - d, j)

        for src in range(nz):
            await_chunk(src, 1 - c, j)

    def produce(j):
        at = chunk(j)
        w = jnp.concatenate([wd[s, i, at, :] for s in range(nz) for i in range(CORES)], axis=1)

        def rows_of(b):
            return lax.dot_general(
                hbuf[b], w, (((1,), (1,)), ((), ())), preferred_element_type=jnp.float32
            )

        ysend[j, diagonal] = rows_of(diagonal).astype(jnp.bfloat16)
        back(0, j).start()
        back(1, j).start()
        y = rows_of(across)
        ysend[j, across, :half] = y[:half].astype(jnp.bfloat16)
        keep[j, 1] = y[half:]
        back(2, j).start()
        y = rows_of(along)
        ysend[j, along, half:] = y[half:].astype(jnp.bfloat16)
        keep[j, 0] = y[:half]
        back(3, j).start()
        own[:, at] = rows_of(me)

    def pass_on(j):
        back(0, j).wait_recv()
        v = keep[j, 0] + relay[j, 0].astype(jnp.float32)
        ysend[j, along, :half] = v.astype(jnp.bfloat16)
        back(4, j).start()
        back(1, j).wait_recv()
        v = keep[j, 1] + relay[j, 1].astype(jnp.float32)
        ysend[j, across, half:] = v.astype(jnp.bfloat16)
        back(5, j).start()

    def combine(j):
        for k in range(2, 6):
            back(k, j).wait_recv()
        at = chunk(j)
        total = side[:, at] + own[:, at]
        for k in range(2):
            total = total + yrecv[j, k].astype(jnp.float32)
        out_ref[:, at] = total.astype(jnp.bfloat16)

    def step(j, carry):
        with jax.named_scope("take"):
            take(j)
        with jax.named_scope("produce"):
            produce(j)

        @pl.when(j >= 1)
        def _():
            with jax.named_scope("pass_on"):
                pass_on(j - 1)

        @pl.when((j >= 2) & (j < nj - 1))
        def _():
            with jax.named_scope("combine"):
                combine(j - 2)

        return carry

    lax.fori_loop(0, nj, step, 0)
    with jax.named_scope("pass_on"):
        pass_on(nj - 1)
    for j in range(nj - 3, nj):
        with jax.named_scope("combine"):
            combine(j)

    drain = jax.named_scope("drain")
    drain.__enter__()
    for k in range(4):
        token_copy(k).wait_send()
    for k in range(ne - 1):
        gate_copy(k, me).wait_send()
        for p in range(3):
            dense_copy(k, p, me).wait_send()
            dense_partner(k, p, c).wait_send()
    for src in range(nz):
        @pl.when((z < nz - 1) & (z >= src))
        def _():
            for p in range(2):
                to_right(src, p).wait_send()
            await_sent(src, cright)

        @pl.when((z > 0) & (z <= src))
        def _():
            for p in range(2):
                to_left(src, p).wait_send()
            await_sent(src, cleft)

        for p in range(2):
            to_partner(src, p).wait_send()
        await_sent(src, cpartner)
    for k in range(6):
        await_back(k)
    drain.__exit__(None, None, None)


def dense_side(ne, me, xg, dgs, dus, dds, mix_ref, side):
    deep, wide = dgs.shape[1], dds.shape[2]
    g = u = None
    for e in range(ne):
        x = xg[me, :, e * deep : (e + 1) * deep]
        ge = jnp.dot(x, dgs[e], preferred_element_type=jnp.float32)
        ue = jnp.dot(x, dus[e], preferred_element_type=jnp.float32)
        g, u = (ge, ue) if e == 0 else (g + ge, u + ue)
    h = (g / (1.0 + jnp.exp(-g)) * u).astype(jnp.bfloat16)
    for e in range(ne):
        o = jnp.dot(h, dds[e], preferred_element_type=jnp.float32)
        side[:, e * wide : (e + 1) * wide] = mix_ref[...] * o


def fused_layer(
    ne, tp, tokens, norm_gain, expert_ids, gate_weights,
    w_gate, w_up, w_down, dense_gate, dense_up, dense_down, mix_vector,
):
    nz = tp // CORES
    rows, width = tokens.shape
    shard = w_gate.shape[2]
    nj = width // CHUNK
    half = rows // 2
    bf, f32 = jnp.bfloat16, jnp.float32
    dma = pltpu.SemaphoreType.DMA
    hbm = pl.BlockSpec(memory_space=pl.ANY)
    vmem = pl.BlockSpec(memory_space=pltpu.VMEM)
    flops = 6 * ne * rows * width * shard * tp
    return pl.pallas_call(
        functools.partial(moe_kernel, ne, nz),
        out_shape=pltpu.VMEM((rows, width), bf),
        in_specs=[hbm] * 7 + [vmem] * 4,
        out_specs=vmem,
        scratch_shapes=[
            pltpu.VMEM((rows, width), bf),
            pltpu.VMEM((ne, rows, width), bf),
            pltpu.VMEM((nz, CORES, 2, width, shard), bf),
            pltpu.VMEM((nz, CORES, width, shard), bf),
            pltpu.VMEM((ne,) + dense_gate.shape, bf),
            pltpu.VMEM((ne,) + dense_up.shape, bf),
            pltpu.VMEM((ne,) + dense_down.shape, bf),
            pltpu.VMEM((ne, rows, tp * shard), bf),
            pltpu.VMEM((rows, width), f32),
            pltpu.VMEM((nj, 2, half, CHUNK), f32),
            pltpu.VMEM((nj, ne, rows, CHUNK), bf),
            pltpu.VMEM((nj, 2, rows, CHUNK), bf),
            pltpu.VMEM((nj, 2, half, CHUNK), bf),
            pltpu.VMEM((rows, width), f32),
            pltpu.VMEM((rows, 1), f32),
            pltpu.VMEM((ne, SUB, rows), f32),
            pltpu.VMEM((ne, rows, 1), f32),
            dma((7,)),
            dma((nz, CORES, 2)),
            dma((nz, 2)),
            dma((nz, 2)),
            dma((nz, 2)),
            dma((nj, nz, CORES)),
            dma((nz,)),
            dma((nz,)),
            dma((nz,)),
            dma((4,)),
            dma((4,)),
            dma((ne,)),
            dma((ne,)),
            dma((ne, 3)),
            dma((ne, 3)),
            dma((ne, 3)),
            dma((ne, 3)),
            dma((6,)),
            dma((nj, 6)),
        ],
        compiler_params=pltpu.CompilerParams(
            collective_id=0, has_side_effects=True, vmem_limit_bytes=VMEM_BYTES
        ),
        cost_estimate=pl.CostEstimate(
            flops=flops, bytes_accessed=8 * rows * width, transcendentals=ne * rows * shard * tp
        ),
    )(
        tokens, w_gate[0], w_up[0], w_down[0], dense_gate, dense_up, dense_down,
        expert_ids.T, gate_weights.T, norm_gain.reshape(1, width), mix_vector.reshape(1, width),
    )


def fits(ne, tp, tokens, w_gate, dense_gate):
    rows, width = tokens.shape
    shard = w_gate.shape[2]
    block = rows * width
    size = 2 * ne * block * 2 + 24 * block + 6 * width * shard * tp
    size += 2 * ne * rows * shard * tp + 6 * ne * dense_gate.size + 1024 * ne * rows
    aligned = shard % 128 == 0 and width % (2 * CHUNK) == 0 and rows % 64 == 0
    return ne == 4 and tp == 4 * CORES and aligned and size < VMEM_BYTES * 15 // 16


def dense_branch(normed, dense_gate, dense_up, dense_down, mix_vector):
    dense_g = jnp.dot(
        normed,
        lax.all_gather(dense_gate, "ep", axis=0, tiled=True),
        preferred_element_type=jnp.float32,
    )
    dense_u = jnp.dot(
        normed,
        lax.all_gather(dense_up, "ep", axis=0, tiled=True),
        preferred_element_type=jnp.float32,
    )
    dense_hidden = (jax.nn.silu(dense_g) * dense_u).astype(jnp.bfloat16)
    dense_out = jnp.dot(
        dense_hidden,
        lax.all_gather(dense_down, "ep", axis=1, tiled=True),
        preferred_element_type=jnp.float32,
    )
    mix = jax.nn.sigmoid(jnp.sum(normed.astype(jnp.float32) * mix_vector, axis=1))
    return mix[:, None] * dense_out


def on_device(
    tokens,
    norm_gain,
    expert_ids,
    gate_weights,
    w_gate,
    w_up,
    w_down,
    dense_gate,
    dense_up,
    dense_down,
    mix_vector,
):
    groups = lax.axis_size("ep")
    ring = lax.axis_size("tp")
    if fits(groups, ring, tokens, w_gate, dense_gate):
        return fused_layer(
            groups, ring, tokens, norm_gain, expert_ids, gate_weights,
            w_gate, w_up, w_down, dense_gate, dense_up, dense_down, mix_vector,
        )
    values = tokens.astype(jnp.float32)
    scale = lax.rsqrt(jnp.mean(values * values, axis=1, keepdims=True) + eps)
    normed = (values * scale * norm_gain).astype(jnp.bfloat16)
    count_tok, topk = expert_ids.shape
    width = tokens.shape[1]
    capacity = 2 * count_tok * topk // groups
    flat_ids = expert_ids.reshape(-1)
    onehot = (flat_ids[:, None] == jnp.arange(groups, dtype=jnp.int32)[None, :]).astype(jnp.int32)
    before = jnp.cumsum(onehot, axis=0) - onehot
    slot = jnp.sum(before * onehot, axis=1)
    dest = flat_ids * capacity + slot
    owner = jnp.arange(count_tok * topk, dtype=jnp.int32) // topk
    buffer = jnp.zeros((groups * capacity, width), jnp.bfloat16).at[dest].set(normed[owner])
    arrived = lax.all_to_all(
        buffer.reshape(groups, capacity, width), "ep", split_axis=0, concat_axis=0, tiled=True
    )
    rows = arrived.reshape(groups * capacity, width)
    gate = jnp.dot(
        rows,
        lax.all_gather(w_gate, "tp", axis=2, tiled=True)[0],
        preferred_element_type=jnp.float32,
    )
    upper = jnp.dot(
        rows, lax.all_gather(w_up, "tp", axis=2, tiled=True)[0], preferred_element_type=jnp.float32
    )
    hidden_all = (jax.nn.silu(gate) * upper).astype(jnp.bfloat16)
    expert_out = lax.dot_general(
        hidden_all,
        lax.all_gather(w_down, "tp", axis=2, tiled=True)[0],
        (((1,), (1,)), ((), ())),
        preferred_element_type=jnp.float32,
    )
    results = expert_out.astype(jnp.bfloat16).reshape(groups, capacity, width)
    returned = lax.all_to_all(results, "ep", split_axis=0, concat_axis=0, tiled=True)
    picked = returned.reshape(groups * capacity, width)[dest].reshape(count_tok, topk, width)
    routed = jnp.einsum("tk,tkd->td", gate_weights, picked.astype(jnp.float32))
    side = dense_branch(normed, dense_gate, dense_up, dense_down, mix_vector)
    return (routed + side).astype(jnp.bfloat16)


def solution(mesh):
    placed = (
        P(("ep", "tp"), None),
        P(),
        P(("ep", "tp"), None),
        P(("ep", "tp"), None),
        P("ep", None, "tp"),
        P("ep", None, "tp"),
        P("ep", None, "tp"),
        P("ep", None),
        P("ep", None),
        P(None, "ep"),
        P(),
    )
    return jax.shard_map(
        on_device, mesh=mesh, in_specs=placed, out_specs=P(("ep", "tp"), None), check_vma=False
    )
```

```python
import functools

import jax
import jax.numpy as jnp
from jax import lax
from jax.experimental import pallas as pl
from jax.experimental.pallas import tpu as pltpu
from jax.sharding import PartitionSpec as P

MESH = pl.DeviceIdType.MESH
VMEM_BYTES = 64000 * 1024
CORES = 2
UNIT = 128
SUB = 8
eps = 1e-06


def moe_kernel(
    ne, nz, x_hbm, wg_hbm, wu_hbm, wd_hbm, dg_hbm, du_hbm, dd_hbm, ids_hbm, gates_hbm,
    gain_hbm, mixv_hbm, out_ref,
    xin, xg, ws, dgs, dus, dds, gbuf, hbuf, own, keep, ysend, yrecv, relay, side, mix_ref, wts, wcol,
    ids_ref, gates_ref, gain_ref, mixv_ref,
    lsem, wrecv, wright, wleft, wpartner, crecv, precv,
    tsend, trecv, gsem, dsem, drecv, rsend, rrecv,
):
    me = lax.axis_index("ep")
    tp = lax.axis_index("tp")
    z = tp // CORES
    c = tp % CORES
    rows, width = xg.shape[1], xg.shape[2]
    units = ysend.shape[2]
    nj = crecv.shape[0]
    half = rows // 2
    shard = ws.shape[4]
    across, along, diagonal = me + 1 - 2 * (me % 2), (me + 2) % ne, ne - 1 - me
    peers = [across, along, diagonal]
    partner = z * CORES + (1 - c)

    local = [pltpu.make_async_copy(wg_hbm, ws.at[z, c, 0], lsem.at[0])]
    local.append(pltpu.make_async_copy(wu_hbm, ws.at[z, c, 1], lsem.at[1]))
    local.append(pltpu.make_async_copy(x_hbm, xin, lsem.at[2]))
    local.append(pltpu.make_async_copy(wd_hbm, ws.at[z, c, 2], lsem.at[3]))
    for p, (ref, slot) in enumerate(((dg_hbm, dgs), (du_hbm, dus), (dd_hbm, dds))):
        local.append(pltpu.make_async_copy(ref, slot.at[0], lsem.at[4 + p]))
    smalls = ((ids_hbm, ids_ref), (gates_hbm, gates_ref), (gain_hbm, gain_ref), (mixv_hbm, mixv_ref))
    for p, (ref, slot) in enumerate(smalls):
        local.append(pltpu.make_async_copy(ref, slot, lsem.at[7 + p]))
    for copy in local:
        copy.start()

    barrier = pltpu.get_barrier_semaphore()
    for peer in peers:
        pl.semaphore_signal(barrier, inc=1, device_id={"ep": peer}, device_id_type=MESH)
    pl.semaphore_signal(barrier, inc=1, device_id={"tp": partner}, device_id_type=MESH)

    @pl.when(z > 0)
    def _():
        pl.semaphore_signal(barrier, inc=1, device_id={"tp": tp - CORES}, device_id_type=MESH)

    @pl.when(z < nz - 1)
    def _():
        pl.semaphore_signal(barrier, inc=1, device_id={"tp": tp + CORES}, device_id_type=MESH)

    neighbours = (z + nz - 1) // nz + (2 * nz - 2 - z) // nz
    with jax.named_scope("barrier"):
        pl.semaphore_wait(barrier, ne + neighbours)

    def remote(src, dst, send, recv, **device):
        return pltpu.make_async_remote_copy(
            src_ref=src, dst_ref=dst, send_sem=send, recv_sem=recv,
            device_id=device, device_id_type=MESH,
        )

    def weight_copy(src, p, target, sems):
        piece = ws.at[src, c, p]
        return remote(piece, piece, sems.at[src], wrecv.at[src, c, p], tp=target)

    def to_right(src, p):
        weight_copy(src, p, tp + CORES, wright).start()

    def to_left(src, p):
        weight_copy(src, p, tp - CORES, wleft).start()

    def to_partner(src, p):
        weight_copy(src, p, partner, wpartner).start()

    def await_piece(src, color, p):
        piece = ws.at[src, color, p]
        remote(piece, piece, wpartner.at[src], wrecv.at[src, color, p], tp=partner).wait_recv()

    def await_sent(src, sems):
        piece = ws.at[src, c]
        remote(piece, piece, sems.at[src], wrecv.at[src, c, 0], tp=partner).wait_send()

    def at(j, fn):
        if isinstance(j, int):
            if 0 <= j < nj:
                fn(j, max(2 * j - 1, 0), 1 if j in (0, nj - 1) else 2)
            return
        pl.when(j == 0)(lambda: fn(0, 0, 1))
        pl.when((j > 0) & (j < nj - 1))(lambda: fn(j, 2 * j - 1, 2))
        pl.when(j == nj - 1)(lambda: fn(nj - 1, units - 1, 1))

    def columns(u, n):
        return pl.ds(pl.multiple_of(u * UNIT, UNIT), n * UNIT)

    def chunk_copy(src, target, sems, recv, u, n):
        piece = ws.at[src, c, 2, columns(u, n)]
        remote(piece, piece, sems.at[src], recv, tp=target).start()

    def c_right(src, j, u, n):
        chunk_copy(src, tp + CORES, wright, crecv.at[j, src], u, n)

    def c_left(src, j, u, n):
        chunk_copy(src, tp - CORES, wleft, crecv.at[j, src], u, n)

    def c_partner(src, j, u, n):
        chunk_copy(src, partner, wpartner, precv.at[j], u, n)

    def arrive(src, j, u, n):
        piece = ws.at[src, c, 2, columns(u, n)]
        remote(piece, piece, wpartner.at[src], crecv.at[j, src], tp=partner).wait_recv()
        c_partner(src, j, u, n)

    def token_copy(k):
        block = (me, me, across, along)[k]
        peer = (across, along, along, across)[k]
        low, size = ((0, rows), (0, rows), (0, half), (half, half))[k]
        piece = xg.at[block, low : low + size]
        return remote(piece, piece, tsend.at[k], trecv.at[k], ep=peer)

    def await_token(k):
        block = (across, along, diagonal, diagonal)[k]
        low, size = ((0, rows), (0, rows), (0, half), (half, half))[k]
        piece = xg.at[block, low : low + size]
        remote(piece, piece, tsend.at[k], trecv.at[k], ep=across).wait_recv()

    def gate_copy(k):
        return remote(wts.at[0], wts.at[1 + k], gsem.at[0], gsem.at[1 + k], ep=peers[k])

    def gate_all():
        piece = wts.at[1:]
        return remote(piece, piece, gsem.at[0], gsem.at[1], ep=across)

    def await_gate(k):
        piece = wts.at[1 + k]
        remote(piece, piece, gsem.at[0], gsem.at[1 + k], ep=across).wait_recv()

    def dense_piece(p, blocks, color):
        slot = (dgs, dus, dds)[p]
        part = slot.shape[1] // CORES
        return slot.at[blocks, pl.ds(pl.multiple_of(color * part, part), part)]

    def dense_copy(k, p):
        lands = dense_piece(p, 1 + k, c)
        return remote(dense_piece(p, 0, c), lands, dsem.at[p], drecv.at[k, p], ep=peers[k])

    def dense_partner(k, p, color):
        piece = dense_piece(p, 1 + k, color)
        return remote(piece, piece, dsem.at[3 + p], drecv.at[ne - 1 + k, p], tp=partner)

    def dense_sent(p):
        piece = dense_piece(p, pl.ds(1, ne - 1), c)
        for first in (0, 3):
            remote(piece, piece, dsem.at[first + p], drecv.at[0, p], tp=partner).wait_send()

    for p in range(2):
        local[p].wait()

        @pl.when(z < nz - 1)
        def _():
            to_right(z, p)

        @pl.when(z > 0)
        def _():
            to_left(z, p)

        to_partner(z, p)
    for p in (2, 7, 8, 9, 10):
        local[p].wait()

    expert = lax.broadcasted_iota(jnp.int32, (SUB, rows), 0)
    named, gate = ids_ref[...], gates_ref[...]
    weight = jnp.zeros((SUB, rows), jnp.float32)
    for k in range(ids_ref.shape[0]):
        weight += jnp.where(named[k : k + 1, :] == expert, gate[k : k + 1, :], 0.0)
    wts[0] = weight
    tile = 32

    def norm(i, carry):
        at = pl.ds(pl.multiple_of(i * tile, tile), tile)
        v = xin[at, :].astype(jnp.float32)
        scale = lax.rsqrt(jnp.sum(v * v, axis=1, keepdims=True) * (1.0 / width) + eps)
        n = (v * scale * gain_ref[...]).astype(jnp.bfloat16)
        xg[me, at, :] = n
        m = jnp.sum(n.astype(jnp.float32) * mixv_ref[...], axis=1, keepdims=True)
        mix_ref[at, :] = 1.0 / (1.0 + jnp.exp(-m))
        return carry

    with jax.named_scope("norm"):
        lax.fori_loop(0, rows // tile, norm, 0)
    local[3].wait()

    def own_chunk(j, u, n):
        c_partner(z, j, u, n)

        @pl.when(z == 0)
        def _():
            c_right(z, j, u, n)

        @pl.when(z == nz - 1)
        def _():
            c_left(z, j, u, n)

    def own_chunks(j, carry):
        at(j, own_chunk)
        return carry

    lax.fori_loop(0, nj, own_chunks, 0)
    for k in range(2):
        token_copy(k).start()
    for k in range(ne - 1):
        gate_copy(k).start()

    def forward(d, p):
        @pl.when(z >= d)
        def _():
            await_piece(z - d, c, p)

            @pl.when(z < nz - 1)
            def _():
                to_right(z - d, p)

            to_partner(z - d, p)

        @pl.when(z + d < nz)
        def _():
            await_piece(z + d, c, p)

            @pl.when(z > 0)
            def _():
                to_left(z + d, p)

            to_partner(z + d, p)

    def weight_of(src, p):
        return jnp.concatenate([ws[src, i, p] for i in range(CORES)], axis=1)

    def gate_part(src):
        await_piece(src, 1 - c, 0)

        def one(b, carry):
            g = jnp.dot(xg[b], weight_of(src, 0), preferred_element_type=jnp.float32)
            gbuf[b] = g / (1.0 + jnp.exp(-g)) * wcol[b]
            return carry

        lax.fori_loop(0, ne, one, 0)

    def up_part(src):
        await_piece(src, 1 - c, 1)
        here = pl.ds(pl.multiple_of(src * (CORES * shard), CORES * shard), CORES * shard)

        def one(b, carry):
            u = jnp.dot(xg[b], weight_of(src, 1), preferred_element_type=jnp.float32)
            hbuf[b, :, here] = (gbuf[b] * u).astype(jnp.bfloat16)
            return carry

        lax.fori_loop(0, ne, one, 0)

    def hidden(src):
        gate_part(src)
        up_part(src)

    def both(d, fn):
        @pl.when(z >= d)
        def _():
            fn(z - d)

        @pl.when(z + d < nz)
        def _():
            fn(z + d)

    def ahead(t):
        def one(d, j, u, n):
            @pl.when(z == 1)
            def _():
                if d == 0:
                    c_right(z, j, u, n)
                elif d == 1:
                    arrive(z - 1, j, u, n)
                    c_right(z - 1, j, u, n)
                    arrive(z + 1, j, u, n)
                else:
                    arrive(z + 2, j, u, n)
                    for src in range(nz - 1):
                        c_left(z + src, j, u, n)

            @pl.when(z == 2)
            def _():
                if d == 0:
                    c_left(z, j, u, n)
                elif d == 1:
                    arrive(z + 1, j, u, n)
                    c_left(z + 1, j, u, n)
                    arrive(z - 1, j, u, n)
                else:
                    arrive(z - 2, j, u, n)
                    for src in range(nz - 1):
                        c_right(z - src, j, u, n)

        for d in range(nz - 1):
            at(t + nz - 1 - d, functools.partial(one, d))

    for p in range(2):
        with jax.named_scope(f"forward1_{p}"):
            forward(1, p)
    with jax.named_scope("token_relay"):
        for k in range(2):
            await_token(k)
            token_copy(2 + k).start()
    for p in range(3):
        local[4 + p].wait()
        for k in range(ne - 1):
            dense_copy(k, p).start()
    for d in range(2, nz - 1):
        for p in range(2):
            with jax.named_scope(f"forward{d}_{p}"):
                forward(d, p)
    ahead(1 - nz)
    with jax.named_scope("gate_wait"):
        for k in range(ne - 1):
            await_gate(k)
    lane = lax.broadcasted_iota(jnp.int32, (rows, SUB), 1)
    for r, b in enumerate([me] + peers):
        column = jnp.where(lane == me, wts[r].T, 0.0)
        wcol[b] = jnp.sum(column, axis=1, keepdims=True)
    with jax.named_scope("token_wait"):
        for k in range(2, 4):
            await_token(k)
    with jax.named_scope("hidden_own"):
        hidden(z)
    for d in range(1, nz - 1):
        with jax.named_scope(f"ahead{d}"):
            ahead(d + 1 - nz)
        with jax.named_scope(f"hidden{d}"):
            both(d, hidden)
    with jax.named_scope("dense_wait"):
        for p in range(3):
            for k in range(ne - 1):
                dense_copy(k, p).wait_recv()
                dense_partner(k, p, c).start()
    with jax.named_scope("forward_last0"):
        forward(nz - 1, 0)
    with jax.named_scope("gate_last"):
        both(nz - 1, gate_part)
    with jax.named_scope("dense_partner"):
        for p in range(3):
            for k in range(ne - 1):
                dense_partner(k, p, 1 - c).wait_recv()
    with jax.named_scope("dense_side"):
        dense_side([me] + peers, me, xg, dgs, dus, dds, mix_ref, side)
    with jax.named_scope("forward_last1"):
        forward(nz - 1, 1)
    with jax.named_scope("up_last"):
        both(nz - 1, up_part)

    def back(k, j, u, n):
        block = (diagonal, diagonal, across, along, along, across)[k]
        peer = (across, along, across, along, along, across)[k]
        spot = (0, 1, 0, 1, 1, 0)[k]
        to = pl.ds(u, n)
        lands = relay.at[k, to] if k < 2 else yrecv.at[spot, k % 2, to]
        piece = ysend.at[block, k % 2, to]
        return remote(piece, lands, rsend.at[0], rrecv.at[j, min(k, 2)], ep=peer)

    def await_back(j, u, n):
        piece = yrecv.at[:, :, pl.ds(u, n)]
        remote(piece, piece, rsend.at[0], rrecv.at[j, 2], ep=across).wait_recv()

    def take(j, u, n):
        ahead(j)

        @pl.when(z == 0)
        def _():
            for d in range(1, nz):
                arrive(d, j, u, n)

        @pl.when(z == nz - 1)
        def _():
            for d in range(1, nz):
                arrive(z - d, j, u, n)

        piece = ws.at[:, 1 - c, 2, columns(u, n)]
        remote(piece, piece, wpartner.at[0], precv.at[j], tp=partner).wait_recv()

    def produce(j, u, n):
        here = columns(u, n)
        w = jnp.concatenate([ws[s, i, 2, here, :] for s in range(nz) for i in range(CORES)], axis=1)

        def rows_of(b):
            return lax.dot_general(
                hbuf[b], w, (((1,), (1,)), ((), ())), preferred_element_type=jnp.float32
            )

        def put(y, *lead):
            ref, lead = lead[0], lead[1:]
            for i in range(n):
                ref[lead + (u + i,)] = y[:, i * UNIT : (i + 1) * UNIT].astype(ref.dtype)

        y = rows_of(diagonal)
        for k in range(2):
            put(y[k * half : (k + 1) * half], ysend, diagonal, k)
            back(k, j, u, n).start()
        y = rows_of(across)
        put(y[:half], ysend, across, 0)
        put(y[half:], keep, 1)
        back(2, j, u, n).start()
        y = rows_of(along)
        put(y[half:], ysend, along, 1)
        put(y[:half], keep, 0)
        back(3, j, u, n).start()
        own[:, here] = rows_of(me)

    def pass_on(j, u, n):
        for k, block in enumerate((along, across)):
            back(k, j, u, n).wait_recv()
            for i in range(n):
                v = keep[k, u + i] + relay[k, u + i].astype(jnp.float32)
                ysend[block, k, u + i] = v.astype(jnp.bfloat16)
            back(4 + k, j, u, n).start()

    def combine(j, u, n):
        await_back(j, u, n)
        for i in range(n):
            here = columns(u + i, 1)
            for h in range(2):
                low = h * half
                total = side[low : low + half, here] + own[low : low + half, here]
                for k in range(2):
                    total = total + yrecv[k, h, u + i].astype(jnp.float32)
                out_ref[low : low + half, here] = total.astype(jnp.bfloat16)

    def scoped(name, j, fn):
        with jax.named_scope(name):
            at(j, fn)

    def step(j, carry):
        take(j, 2 * j - 1, 2)
        with jax.named_scope("produce"):
            produce(j, 2 * j - 1, 2)
        scoped("pass_on", j - 1, pass_on)
        scoped("combine", j - 2, combine)
        return carry

    scoped("take", 0, take)
    scoped("produce", 0, produce)
    lax.fori_loop(1, nj - 1, step, 0)
    scoped("take", nj - 1, take)
    scoped("produce", nj - 1, produce)
    scoped("pass_on", nj - 2, pass_on)
    scoped("pass_on", nj - 1, pass_on)
    for j in range(nj - 3, nj):
        scoped("combine", j, combine)

    drain = jax.named_scope("drain")
    drain.__enter__()
    for k in range(4):
        token_copy(k).wait_send()
    gate_all().wait_send()
    for p in range(3):
        dense_sent(p)
    for src in range(nz):
        @pl.when((z < nz - 1) & (z >= src))
        def _():
            await_sent(src, wright)

        @pl.when((z > 0) & (z <= src))
        def _():
            await_sent(src, wleft)

        await_sent(src, wpartner)
    piece = ysend.at[: ne - 1]
    remote(piece, piece, rsend.at[0], rrecv.at[0, 0], ep=across).wait_send()
    drain.__exit__(None, None, None)


def dense_side(owners, me, xg, dgs, dus, dds, mix_ref, side):
    deep, wide = dgs.shape[1], dds.shape[2]
    g = u = None
    for r, e in enumerate(owners):
        x = xg[me, :, pl.ds(pl.multiple_of(e * deep, deep), deep)]
        ge = jnp.dot(x, dgs[r], preferred_element_type=jnp.float32)
        ue = jnp.dot(x, dus[r], preferred_element_type=jnp.float32)
        g, u = (ge, ue) if r == 0 else (g + ge, u + ue)
    h = (g / (1.0 + jnp.exp(-g)) * u).astype(jnp.bfloat16)
    for r, e in enumerate(owners):
        o = jnp.dot(h, dds[r], preferred_element_type=jnp.float32)
        side[:, pl.ds(pl.multiple_of(e * wide, wide), wide)] = mix_ref[...] * o


def fused_layer(
    ne, tp, tokens, norm_gain, expert_ids, gate_weights,
    w_gate, w_up, w_down, dense_gate, dense_up, dense_down, mix_vector,
):
    nz = tp // CORES
    rows, width = tokens.shape
    topk = expert_ids.shape[1]
    shard = w_gate.shape[2]
    units = width // UNIT
    nj = units // 2 + 1
    half = rows // 2
    bf, f32 = jnp.bfloat16, jnp.float32
    dma = pltpu.SemaphoreType.DMA
    hbm = pl.BlockSpec(memory_space=pl.ANY)
    vmem = pl.BlockSpec(memory_space=pltpu.VMEM)
    flops = 6 * ne * rows * width * shard * tp
    return pl.pallas_call(
        functools.partial(moe_kernel, ne, nz),
        out_shape=pltpu.VMEM((rows, width), bf),
        in_specs=[hbm] * 11,
        out_specs=vmem,
        scratch_shapes=[
            pltpu.VMEM((rows, width), bf),
            pltpu.VMEM((ne, rows, width), bf),
            pltpu.VMEM((nz, CORES, 3, width, shard), bf),
            pltpu.VMEM((ne,) + dense_gate.shape, bf),
            pltpu.VMEM((ne,) + dense_up.shape, bf),
            pltpu.VMEM((ne,) + dense_down.shape, bf),
            pltpu.VMEM((ne, rows, CORES * shard), f32),
            pltpu.VMEM((ne, rows, tp * shard), bf),
            pltpu.VMEM((rows, width), f32),
            pltpu.VMEM((2, units, half, UNIT), f32),
            pltpu.VMEM((ne, 2, units, half, UNIT), bf),
            pltpu.VMEM((2, 2, units, half, UNIT), bf),
            pltpu.VMEM((2, units, half, UNIT), bf),
            pltpu.VMEM((rows, width), f32),
            pltpu.VMEM((rows, 1), f32),
            pltpu.VMEM((ne, SUB, rows), f32),
            pltpu.VMEM((ne, rows, 1), f32),
            pltpu.VMEM((topk, rows), jnp.int32),
            pltpu.VMEM((topk, rows), f32),
            pltpu.VMEM((1, width), f32),
            pltpu.VMEM((1, width), f32),
            dma((11,)),
            dma((nz, CORES, 2)),
            dma((nz,)),
            dma((nz,)),
            dma((nz,)),
            dma((nj, nz)),
            dma((nj,)),
            dma((4,)),
            dma((4,)),
            dma((ne,)),
            dma((6,)),
            dma((2 * ne - 2, 3)),
            dma((1,)),
            dma((nj, 3)),
        ],
        compiler_params=pltpu.CompilerParams(
            collective_id=0, has_side_effects=True, vmem_limit_bytes=VMEM_BYTES
        ),
        cost_estimate=pl.CostEstimate(
            flops=flops, bytes_accessed=8 * rows * width, transcendentals=ne * rows * shard * tp
        ),
    )(
        tokens, w_gate[0], w_up[0], w_down[0], dense_gate, dense_up, dense_down,
        expert_ids.T, gate_weights.T, norm_gain.reshape(1, width), mix_vector.reshape(1, width),
    )


def fits(ne, tp, tokens, w_gate, dense_gate):
    rows, width = tokens.shape
    shard = w_gate.shape[2]
    block = rows * width
    size = 2 * ne * block * 2 + 24 * block + 6 * width * shard * tp
    size += 2 * ne * rows * shard * tp + 6 * ne * dense_gate.size + 1024 * ne * rows
    size += 8 * ne * rows * shard
    aligned = shard % 128 == 0 and width % (2 * UNIT) == 0 and rows % 64 == 0
    return ne == 4 and tp == 4 * CORES and aligned and size < VMEM_BYTES * 15 // 16


def dense_branch(normed, dense_gate, dense_up, dense_down, mix_vector):
    dense_g = jnp.dot(
        normed,
        lax.all_gather(dense_gate, "ep", axis=0, tiled=True),
        preferred_element_type=jnp.float32,
    )
    dense_u = jnp.dot(
        normed,
        lax.all_gather(dense_up, "ep", axis=0, tiled=True),
        preferred_element_type=jnp.float32,
    )
    dense_hidden = (jax.nn.silu(dense_g) * dense_u).astype(jnp.bfloat16)
    dense_out = jnp.dot(
        dense_hidden,
        lax.all_gather(dense_down, "ep", axis=1, tiled=True),
        preferred_element_type=jnp.float32,
    )
    mix = jax.nn.sigmoid(jnp.sum(normed.astype(jnp.float32) * mix_vector, axis=1))
    return mix[:, None] * dense_out


def on_device(
    tokens,
    norm_gain,
    expert_ids,
    gate_weights,
    w_gate,
    w_up,
    w_down,
    dense_gate,
    dense_up,
    dense_down,
    mix_vector,
):
    groups = lax.axis_size("ep")
    ring = lax.axis_size("tp")
    if fits(groups, ring, tokens, w_gate, dense_gate):
        return fused_layer(
            groups, ring, tokens, norm_gain, expert_ids, gate_weights,
            w_gate, w_up, w_down, dense_gate, dense_up, dense_down, mix_vector,
        )
    values = tokens.astype(jnp.float32)
    scale = lax.rsqrt(jnp.mean(values * values, axis=1, keepdims=True) + eps)
    normed = (values * scale * norm_gain).astype(jnp.bfloat16)
    count_tok, topk = expert_ids.shape
    width = tokens.shape[1]
    capacity = 2 * count_tok * topk // groups
    flat_ids = expert_ids.reshape(-1)
    onehot = (flat_ids[:, None] == jnp.arange(groups, dtype=jnp.int32)[None, :]).astype(jnp.int32)
    before = jnp.cumsum(onehot, axis=0) - onehot
    slot = jnp.sum(before * onehot, axis=1)
    dest = flat_ids * capacity + slot
    owner = jnp.arange(count_tok * topk, dtype=jnp.int32) // topk
    buffer = jnp.zeros((groups * capacity, width), jnp.bfloat16).at[dest].set(normed[owner])
    arrived = lax.all_to_all(
        buffer.reshape(groups, capacity, width), "ep", split_axis=0, concat_axis=0, tiled=True
    )
    rows = arrived.reshape(groups * capacity, width)
    gate = jnp.dot(
        rows,
        lax.all_gather(w_gate, "tp", axis=2, tiled=True)[0],
        preferred_element_type=jnp.float32,
    )
    upper = jnp.dot(
        rows, lax.all_gather(w_up, "tp", axis=2, tiled=True)[0], preferred_element_type=jnp.float32
    )
    hidden_all = (jax.nn.silu(gate) * upper).astype(jnp.bfloat16)
    expert_out = lax.dot_general(
        hidden_all,
        lax.all_gather(w_down, "tp", axis=2, tiled=True)[0],
        (((1,), (1,)), ((), ())),
        preferred_element_type=jnp.float32,
    )
    results = expert_out.astype(jnp.bfloat16).reshape(groups, capacity, width)
    returned = lax.all_to_all(results, "ep", split_axis=0, concat_axis=0, tiled=True)
    picked = returned.reshape(groups * capacity, width)[dest].reshape(count_tok, topk, width)
    routed = jnp.einsum("tk,tkd->td", gate_weights, picked.astype(jnp.float32))
    side = dense_branch(normed, dense_gate, dense_up, dense_down, mix_vector)
    return (routed + side).astype(jnp.bfloat16)


def solution(mesh):
    placed = (
        P(("ep", "tp"), None),
        P(),
        P(("ep", "tp"), None),
        P(("ep", "tp"), None),
        P("ep", None, "tp"),
        P("ep", None, "tp"),
        P("ep", None, "tp"),
        P("ep", None),
        P("ep", None),
        P(None, "ep"),
        P(),
    )
    return jax.shard_map(
        on_device, mesh=mesh, in_specs=placed, out_specs=P(("ep", "tp"), None), check_vma=False
    )
```

```python
import functools

import jax
import jax.numpy as jnp
from jax import lax
from jax.experimental import pallas as pl
from jax.experimental.pallas import tpu as pltpu
from jax.sharding import PartitionSpec as P

MESH = pl.DeviceIdType.MESH
VMEM_BYTES = 64000 * 1024
CORES = 2
UNIT = 128
TAIL = 256
SUB = 8
eps = 1e-06


def moe_kernel(
    ne, nz, x_hbm, wg_hbm, wu_hbm, wd_hbm, dg_hbm, du_hbm, dd_hbm, ids_hbm, gates_hbm,
    gain_hbm, mixv_hbm, out_ref,
    xin, xg, ws, dgs, dus, dds, gbuf, hbuf, own, keep, ysend, yrecv, relay, side, mix_ref, wts, wcol,
    ids_ref, gates_ref, gain_ref, mixv_ref,
    lsem, wrecv, wright, wleft, wpartner, xsend, xrecv, crecv, precv,
    tsend, trecv, gsem, dsem, drecv, rsend, rrecv,
):
    me = lax.axis_index("ep")
    tp = lax.axis_index("tp")
    z = tp // CORES
    c = tp % CORES
    rows, width = xg.shape[1], xg.shape[2]
    units = ysend.shape[2]
    nj = crecv.shape[0]
    half = rows // 2
    shard = ws.shape[4]
    across, along, diagonal = me + 1 - 2 * (me % 2), (me + 2) % ne, ne - 1 - me
    peers = [across, along, diagonal]
    partner = z * CORES + (1 - c)

    local = [pltpu.make_async_copy(wg_hbm, ws.at[z, c, 0], lsem.at[0])]
    local.append(pltpu.make_async_copy(wu_hbm, ws.at[z, c, 1], lsem.at[1]))
    local.append(pltpu.make_async_copy(x_hbm, xin, lsem.at[2]))
    local.append(pltpu.make_async_copy(wd_hbm, ws.at[z, c, 2], lsem.at[3]))
    for p, (ref, slot) in enumerate(((dg_hbm, dgs), (du_hbm, dus), (dd_hbm, dds))):
        local.append(pltpu.make_async_copy(ref, slot.at[0], lsem.at[4 + p]))
    smalls = ((ids_hbm, ids_ref), (gates_hbm, gates_ref), (gain_hbm, gain_ref), (mixv_hbm, mixv_ref))
    for p, (ref, slot) in enumerate(smalls):
        local.append(pltpu.make_async_copy(ref, slot, lsem.at[7 + p]))
    for copy in local:
        copy.start()

    barrier = pltpu.get_barrier_semaphore()
    for peer in (across, along):
        pl.semaphore_signal(barrier, inc=1, device_id={"ep": peer}, device_id_type=MESH)
    pl.semaphore_signal(barrier, inc=1, device_id={"tp": partner}, device_id_type=MESH)

    @pl.when(z > 0)
    def _():
        pl.semaphore_signal(barrier, inc=1, device_id={"tp": tp - CORES}, device_id_type=MESH)

    @pl.when(z < nz - 1)
    def _():
        pl.semaphore_signal(barrier, inc=1, device_id={"tp": tp + CORES}, device_id_type=MESH)

    neighbours = (z + nz - 1) // nz + (2 * nz - 2 - z) // nz
    with jax.named_scope("barrier"):
        pl.semaphore_wait(barrier, 3 + neighbours)

    def remote(src, dst, send, recv, **device):
        return pltpu.make_async_remote_copy(
            src_ref=src, dst_ref=dst, send_sem=send, recv_sem=recv,
            device_id=device, device_id_type=MESH,
        )

    def weight_copy(src, p, target, sems):
        piece = ws.at[src, c, p]
        return remote(piece, piece, sems.at[src], wrecv.at[src, c, p], tp=target)

    def to_right(src, p):
        weight_copy(src, p, tp + CORES, wright).start()

    def to_left(src, p):
        weight_copy(src, p, tp - CORES, wleft).start()

    def to_partner(src, p):
        weight_copy(src, p, partner, wpartner).start()

    def await_piece(src, color, p):
        piece = ws.at[src, color, p]
        remote(piece, piece, wpartner.at[src], wrecv.at[src, color, p], tp=partner).wait_recv()

    def await_sent(src, sems, count):
        piece = ws.at[src, c, :count]
        remote(piece, piece, sems.at[src], wrecv.at[src, c, 0], tp=partner).wait_send()

    def far_main(src, color, target):
        piece = ws.at[src, color, 1] if color else ws.at[src, 0, 1, : width - TAIL]
        return remote(piece, piece, xsend.at[0], wrecv.at[src, color, 1], tp=target)

    def far_tail(src, target):
        piece = ws.at[src, 0, 1, width - TAIL :]
        return remote(piece, piece, xsend.at[1], xrecv.at[0], tp=target)

    def by_color(fn):
        for color in range(CORES):
            pl.when(c == color)(functools.partial(fn, color))

    def at(j, fn):
        if isinstance(j, int):
            if 0 <= j < nj:
                fn(j, max(2 * j - 1, 0), 1 if j in (0, nj - 1) else 2)
            return
        pl.when(j == 0)(lambda: fn(0, 0, 1))
        pl.when((j > 0) & (j < nj - 1))(lambda: fn(j, 2 * j - 1, 2))
        pl.when(j == nj - 1)(lambda: fn(nj - 1, units - 1, 1))

    def columns(u, n):
        return pl.ds(pl.multiple_of(u * UNIT, UNIT), n * UNIT)

    def chunk_copy(src, target, sems, recv, u, n):
        piece = ws.at[src, c, 2, columns(u, n)]
        remote(piece, piece, sems.at[src], recv, tp=target).start()

    def c_right(src, j, u, n):
        chunk_copy(src, tp + CORES, wright, crecv.at[j, src], u, n)

    def c_left(src, j, u, n):
        chunk_copy(src, tp - CORES, wleft, crecv.at[j, src], u, n)

    def c_partner(src, j, u, n):
        chunk_copy(src, partner, wpartner, precv.at[j], u, n)

    def arrive(src, j, u, n):
        piece = ws.at[src, c, 2, columns(u, n)]
        remote(piece, piece, wpartner.at[src], crecv.at[j, src], tp=partner).wait_recv()
        c_partner(src, j, u, n)

    def token_copy(k):
        block = (me, me, across, along)[k]
        peer = (across, along, along, across)[k]
        low, size = ((0, rows), (0, rows), (0, half), (half, half))[k]
        piece = xg.at[block, low : low + size]
        return remote(piece, piece, tsend.at[k], trecv.at[k], ep=peer)

    def await_token(k):
        block = (across, along, diagonal, diagonal)[k]
        low, size = ((0, rows), (0, rows), (0, half), (half, half))[k]
        piece = xg.at[block, low : low + size]
        remote(piece, piece, tsend.at[k], trecv.at[k], ep=across).wait_recv()

    def gate_copy(k):
        return remote(wts.at[0], wts.at[1 + k], gsem.at[0], gsem.at[1 + k], ep=peers[k])

    def gate_all():
        piece = wts.at[1:]
        return remote(piece, piece, gsem.at[0], gsem.at[1], ep=across)

    def await_gate(k):
        piece = wts.at[1 + k]
        remote(piece, piece, gsem.at[0], gsem.at[1 + k], ep=across).wait_recv()

    def dense_piece(p, blocks, color):
        slot = (dgs, dus, dds)[p]
        part = slot.shape[1] // CORES
        return slot.at[blocks, pl.ds(pl.multiple_of(color * part, part), part)]

    def dense_copy(k, p):
        lands = dense_piece(p, 1 + k, c)
        return remote(dense_piece(p, 0, c), lands, dsem.at[p], drecv.at[k, p], ep=peers[k])

    def dense_partner(k, p, color):
        piece = dense_piece(p, 1 + k, color)
        return remote(piece, piece, dsem.at[3 + p], drecv.at[ne - 1 + k, p], tp=partner)

    def dense_sent(p):
        piece = dense_piece(p, pl.ds(1, ne - 1), c)
        for first in (0, 3):
            remote(piece, piece, dsem.at[first + p], drecv.at[0, p], tp=partner).wait_send()

    for p in range(2):
        local[p].wait()

        @pl.when(z < nz - 1)
        def _():
            to_right(z, p)

        @pl.when(z > 0)
        def _():
            to_left(z, p)

        to_partner(z, p)
    for p in (2, 7, 8, 9, 10):
        local[p].wait()

    expert = lax.broadcasted_iota(jnp.int32, (SUB, rows), 0)
    named, gate = ids_ref[...], gates_ref[...]
    weight = jnp.zeros((SUB, rows), jnp.float32)
    for k in range(ids_ref.shape[0]):
        weight += jnp.where(named[k : k + 1, :] == expert, gate[k : k + 1, :], 0.0)
    wts[0] = weight
    tile = 32

    def norm(i, carry):
        at = pl.ds(pl.multiple_of(i * tile, tile), tile)
        v = xin[at, :].astype(jnp.float32)
        scale = lax.rsqrt(jnp.sum(v * v, axis=1, keepdims=True) * (1.0 / width) + eps)
        n = (v * scale * gain_ref[...]).astype(jnp.bfloat16)
        xg[me, at, :] = n
        m = jnp.sum(n.astype(jnp.float32) * mixv_ref[...], axis=1, keepdims=True)
        mix_ref[at, :] = 1.0 / (1.0 + jnp.exp(-m))
        return carry

    with jax.named_scope("norm"):
        lax.fori_loop(0, rows // tile, norm, 0)
    local[3].wait()

    def own_chunk(j, u, n):
        c_partner(z, j, u, n)

        @pl.when(z == 0)
        def _():
            c_right(z, j, u, n)

        @pl.when(z == nz - 1)
        def _():
            c_left(z, j, u, n)

    def own_chunks(j, carry):
        at(j, own_chunk)
        return carry

    lax.fori_loop(0, nj, own_chunks, 0)
    for k in range(2):
        token_copy(k).start()
    for k in range(2):
        gate_copy(k).start()

    def forward(d, p):
        @pl.when(z >= d)
        def _():
            await_piece(z - d, c, p)

            @pl.when(z < nz - 1)
            def _():
                if d == nz - 2 and p == 1:
                    by_color(lambda color: far_main(z - d, color, tp + CORES).start())
                else:
                    to_right(z - d, p)

            to_partner(z - d, p)

        @pl.when(z + d < nz)
        def _():
            await_piece(z + d, c, p)

            @pl.when(z > 0)
            def _():
                if d == nz - 2 and p == 1:
                    by_color(lambda color: far_main(z + d, color, tp - CORES).start())
                else:
                    to_left(z + d, p)

            to_partner(z + d, p)

    def weight_of(src, p):
        return jnp.concatenate([ws[src, i, p] for i in range(CORES)], axis=1)

    def gate_part(src):
        await_piece(src, 1 - c, 0)

        def one(b, carry):
            g = jnp.dot(xg[b], weight_of(src, 0), preferred_element_type=jnp.float32)
            gbuf[b] = g / (1.0 + jnp.exp(-g)) * wcol[b]
            return carry

        lax.fori_loop(0, ne, one, 0)

    def far_forward():
        src = nz - 1 - z

        def one(color):
            far_main(src, color, partner).wait_recv()
            far_main(src, color, partner).start()
            if color:
                far_tail(src, partner).wait_recv()
                far_tail(src, partner).start()

        by_color(one)

    def far_await(src):
        def one(color):
            far_main(src, 1 - color, partner).wait_recv()
            if not color:
                far_tail(src, partner).wait_recv()

        by_color(one)

    def up_part(src, far=False):
        if far:
            far_await(src)
        else:
            await_piece(src, 1 - c, 1)

            @pl.when((c == 1) & (z == 1) & (src == nz - 1))
            def _():
                far_tail(src, tp - CORES).start()

            @pl.when((c == 1) & (z == nz - 2) & (src == 0))
            def _():
                far_tail(src, tp + CORES).start()

        here = pl.ds(pl.multiple_of(src * (CORES * shard), CORES * shard), CORES * shard)

        def one(b, carry):
            u = jnp.dot(xg[b], weight_of(src, 1), preferred_element_type=jnp.float32)
            hbuf[b, :, here] = (gbuf[b] * u).astype(jnp.bfloat16)
            return carry

        lax.fori_loop(0, ne, one, 0)

    def hidden(src):
        gate_part(src)
        up_part(src)

    def both(d, fn):
        @pl.when(z >= d)
        def _():
            fn(z - d)

        @pl.when(z + d < nz)
        def _():
            fn(z + d)

    def ahead(t):
        def one(d, j, u, n):
            @pl.when(z == 1)
            def _():
                if d == 0:
                    c_right(z, j, u, n)
                elif d == 1:
                    arrive(z - 1, j, u, n)
                    c_right(z - 1, j, u, n)
                    arrive(z + 1, j, u, n)
                else:
                    arrive(z + 2, j, u, n)
                    for src in range(nz - 1):
                        c_left(z + src, j, u, n)

            @pl.when(z == 2)
            def _():
                if d == 0:
                    c_left(z, j, u, n)
                elif d == 1:
                    arrive(z + 1, j, u, n)
                    c_left(z + 1, j, u, n)
                    arrive(z - 1, j, u, n)
                else:
                    arrive(z - 2, j, u, n)
                    for src in range(nz - 1):
                        c_right(z - src, j, u, n)

        for d in range(nz - 1):
            at(t + nz - 1 - d, functools.partial(one, d))

    for p in range(2):
        with jax.named_scope(f"forward1_{p}"):
            forward(1, p)
    with jax.named_scope("token_relay"):
        for k in range(2):
            await_token(k)
            token_copy(2 + k).start()
    gate_copy(2).start()
    for p in range(3):
        local[4 + p].wait()
        for k in range(ne - 1):
            dense_copy(k, p).start()
    for d in range(2, nz - 1):
        for p in range(2):
            with jax.named_scope(f"forward{d}_{p}"):
                forward(d, p)
    ahead(1 - nz)
    with jax.named_scope("gate_wait"):
        for k in range(ne - 1):
            await_gate(k)
    lane = lax.broadcasted_iota(jnp.int32, (rows, SUB), 1)
    for r, b in enumerate([me] + peers):
        column = jnp.where(lane == me, wts[r].T, 0.0)
        wcol[b] = jnp.sum(column, axis=1, keepdims=True)
    with jax.named_scope("token_wait"):
        for k in range(2, 4):
            await_token(k)
    with jax.named_scope("hidden_own"):
        hidden(z)
    for d in range(1, nz - 1):
        with jax.named_scope(f"hidden{d}"):
            both(d, hidden)
        with jax.named_scope(f"ahead{d}"):
            ahead(d + 1 - nz)
    with jax.named_scope("dense_wait"):
        for p in range(3):
            for k in range(ne - 1):
                dense_copy(k, p).wait_recv()
                dense_partner(k, p, c).start()
    with jax.named_scope("forward_last0"):
        forward(nz - 1, 0)
    with jax.named_scope("gate_last"):
        both(nz - 1, gate_part)
    with jax.named_scope("dense_partner"):
        for p in range(3):
            for k in range(ne - 1):
                dense_partner(k, p, 1 - c).wait_recv()
    with jax.named_scope("dense_side"):
        dense_side([me] + peers, me, xg, dgs, dus, dds, mix_ref, side)
    with jax.named_scope("forward_last1"):
        pl.when((z == 0) | (z == nz - 1))(far_forward)
    with jax.named_scope("up_last"):
        both(nz - 1, functools.partial(up_part, far=True))

    def back(k, j, u, n):
        block = (diagonal, diagonal, across, along, along, across)[k]
        peer = (across, along, across, along, along, across)[k]
        spot = (0, 1, 0, 1, 1, 0)[k]
        to = pl.ds(u, n)
        lands = relay.at[k, to] if k < 2 else yrecv.at[spot, k % 2, to]
        piece = ysend.at[block, k % 2, to]
        return remote(piece, lands, rsend.at[0], rrecv.at[j, min(k, 2)], ep=peer)

    def await_back(j, u, n):
        piece = yrecv.at[:, :, pl.ds(u, n)]
        remote(piece, piece, rsend.at[0], rrecv.at[j, 2], ep=across).wait_recv()

    def take(j, u, n):
        ahead(j)

        @pl.when(z == 0)
        def _():
            for d in range(1, nz):
                arrive(d, j, u, n)

        @pl.when(z == nz - 1)
        def _():
            for d in range(1, nz):
                arrive(z - d, j, u, n)

        piece = ws.at[:, 1 - c, 2, columns(u, n)]
        remote(piece, piece, wpartner.at[0], precv.at[j], tp=partner).wait_recv()

    def produce(j, u, n):
        here = columns(u, n)
        w = jnp.concatenate([ws[s, i, 2, here, :] for s in range(nz) for i in range(CORES)], axis=1)

        def rows_of(b):
            return lax.dot_general(
                hbuf[b], w, (((1,), (1,)), ((), ())), preferred_element_type=jnp.float32
            )

        def put(y, *lead):
            ref, lead = lead[0], lead[1:]
            for i in range(n):
                ref[lead + (u + i,)] = y[:, i * UNIT : (i + 1) * UNIT].astype(ref.dtype)

        y = rows_of(diagonal)
        for k in range(2):
            put(y[k * half : (k + 1) * half], ysend, diagonal, k)
            back(k, j, u, n).start()
        y = rows_of(across)
        put(y[:half], ysend, across, 0)
        put(y[half:], keep, 1)
        back(2, j, u, n).start()
        y = rows_of(along)
        put(y[half:], ysend, along, 1)
        put(y[:half], keep, 0)
        back(3, j, u, n).start()
        own[:, here] = rows_of(me)

    def pass_on(j, u, n):
        for k, block in enumerate((along, across)):
            back(k, j, u, n).wait_recv()
            for i in range(n):
                v = keep[k, u + i] + relay[k, u + i].astype(jnp.float32)
                ysend[block, k, u + i] = v.astype(jnp.bfloat16)
            back(4 + k, j, u, n).start()

    def combine(j, u, n):
        await_back(j, u, n)
        for i in range(n):
            here = columns(u + i, 1)
            for h in range(2):
                low = h * half
                total = side[low : low + half, here] + own[low : low + half, here]
                for k in range(2):
                    total = total + yrecv[k, h, u + i].astype(jnp.float32)
                out_ref[low : low + half, here] = total.astype(jnp.bfloat16)

    def scoped(name, j, fn):
        with jax.named_scope(name):
            at(j, fn)

    def step(j, carry):
        take(j, 2 * j - 1, 2)
        with jax.named_scope("produce"):
            produce(j, 2 * j - 1, 2)
        scoped("pass_on", j - 1, pass_on)
        scoped("combine", j - 2, combine)
        return carry

    scoped("take", 0, take)
    scoped("produce", 0, produce)
    lax.fori_loop(1, nj - 1, step, 0)
    scoped("take", nj - 1, take)
    scoped("produce", nj - 1, produce)
    scoped("pass_on", nj - 2, pass_on)
    scoped("pass_on", nj - 1, pass_on)
    for j in range(nj - 3, nj):
        scoped("combine", j, combine)

    drain = jax.named_scope("drain")
    drain.__enter__()
    for k in range(4):
        token_copy(k).wait_send()
    gate_all().wait_send()
    for p in range(3):
        dense_sent(p)
    for src in range(nz):
        for sems, there, far in (
            (wright, (z < nz - 1) & (z >= src), (z == nz - 2) & (src == 0)),
            (wleft, (z > 0) & (z <= src), (z == 1) & (src == nz - 1)),
            (wpartner, z >= 0, (z == nz - 1 - src) & (src % (nz - 1) == 0)),
        ):
            pl.when(there & far)(functools.partial(await_sent, src, sems, 2))
            pl.when(there & jnp.logical_not(far))(functools.partial(await_sent, src, sems, 3))

    def far_sent(color):
        far_main(0, color, partner).wait_send()
        if color:
            far_tail(0, partner).wait_send()

    by_color(far_sent)
    piece = ysend.at[: ne - 1]
    remote(piece, piece, rsend.at[0], rrecv.at[0, 0], ep=across).wait_send()
    drain.__exit__(None, None, None)


def dense_side(owners, me, xg, dgs, dus, dds, mix_ref, side):
    deep, wide = dgs.shape[1], dds.shape[2]
    g = u = None
    for r, e in enumerate(owners):
        x = xg[me, :, pl.ds(pl.multiple_of(e * deep, deep), deep)]
        ge = jnp.dot(x, dgs[r], preferred_element_type=jnp.float32)
        ue = jnp.dot(x, dus[r], preferred_element_type=jnp.float32)
        g, u = (ge, ue) if r == 0 else (g + ge, u + ue)
    h = (g / (1.0 + jnp.exp(-g)) * u).astype(jnp.bfloat16)
    for r, e in enumerate(owners):
        o = jnp.dot(h, dds[r], preferred_element_type=jnp.float32)
        side[:, pl.ds(pl.multiple_of(e * wide, wide), wide)] = mix_ref[...] * o


def fused_layer(
    ne, tp, tokens, norm_gain, expert_ids, gate_weights,
    w_gate, w_up, w_down, dense_gate, dense_up, dense_down, mix_vector,
):
    nz = tp // CORES
    rows, width = tokens.shape
    topk = expert_ids.shape[1]
    shard = w_gate.shape[2]
    units = width // UNIT
    nj = units // 2 + 1
    half = rows // 2
    bf, f32 = jnp.bfloat16, jnp.float32
    dma = pltpu.SemaphoreType.DMA
    hbm = pl.BlockSpec(memory_space=pl.ANY)
    vmem = pl.BlockSpec(memory_space=pltpu.VMEM)
    flops = 6 * ne * rows * width * shard * tp
    return pl.pallas_call(
        functools.partial(moe_kernel, ne, nz),
        out_shape=pltpu.VMEM((rows, width), bf),
        in_specs=[hbm] * 11,
        out_specs=vmem,
        scratch_shapes=[
            pltpu.VMEM((rows, width), bf),
            pltpu.VMEM((ne, rows, width), bf),
            pltpu.VMEM((nz, CORES, 3, width, shard), bf),
            pltpu.VMEM((ne,) + dense_gate.shape, bf),
            pltpu.VMEM((ne,) + dense_up.shape, bf),
            pltpu.VMEM((ne,) + dense_down.shape, bf),
            pltpu.VMEM((ne, rows, CORES * shard), f32),
            pltpu.VMEM((ne, rows, tp * shard), bf),
            pltpu.VMEM((rows, width), f32),
            pltpu.VMEM((2, units, half, UNIT), f32),
            pltpu.VMEM((ne, 2, units, half, UNIT), bf),
            pltpu.VMEM((2, 2, units, half, UNIT), bf),
            pltpu.VMEM((2, units, half, UNIT), bf),
            pltpu.VMEM((rows, width), f32),
            pltpu.VMEM((rows, 1), f32),
            pltpu.VMEM((ne, SUB, rows), f32),
            pltpu.VMEM((ne, rows, 1), f32),
            pltpu.VMEM((topk, rows), jnp.int32),
            pltpu.VMEM((topk, rows), f32),
            pltpu.VMEM((1, width), f32),
            pltpu.VMEM((1, width), f32),
            dma((11,)),
            dma((nz, CORES, 2)),
            dma((nz,)),
            dma((nz,)),
            dma((nz,)),
            dma((2,)),
            dma((1,)),
            dma((nj, nz)),
            dma((nj,)),
            dma((4,)),
            dma((4,)),
            dma((ne,)),
            dma((6,)),
            dma((2 * ne - 2, 3)),
            dma((1,)),
            dma((nj, 3)),
        ],
        compiler_params=pltpu.CompilerParams(
            collective_id=0, has_side_effects=True, vmem_limit_bytes=VMEM_BYTES
        ),
        cost_estimate=pl.CostEstimate(
            flops=flops, bytes_accessed=8 * rows * width, transcendentals=ne * rows * shard * tp
        ),
    )(
        tokens, w_gate[0], w_up[0], w_down[0], dense_gate, dense_up, dense_down,
        expert_ids.T, gate_weights.T, norm_gain.reshape(1, width), mix_vector.reshape(1, width),
    )


def fits(ne, tp, tokens, w_gate, dense_gate):
    rows, width = tokens.shape
    shard = w_gate.shape[2]
    block = rows * width
    size = 2 * ne * block * 2 + 24 * block + 6 * width * shard * tp
    size += 2 * ne * rows * shard * tp + 6 * ne * dense_gate.size + 1024 * ne * rows
    size += 8 * ne * rows * shard
    aligned = shard % 128 == 0 and width % (2 * UNIT) == 0 and width > TAIL and rows % 64 == 0
    return ne == 4 and tp == 4 * CORES and aligned and size < VMEM_BYTES * 15 // 16


def dense_branch(normed, dense_gate, dense_up, dense_down, mix_vector):
    dense_g = jnp.dot(
        normed,
        lax.all_gather(dense_gate, "ep", axis=0, tiled=True),
        preferred_element_type=jnp.float32,
    )
    dense_u = jnp.dot(
        normed,
        lax.all_gather(dense_up, "ep", axis=0, tiled=True),
        preferred_element_type=jnp.float32,
    )
    dense_hidden = (jax.nn.silu(dense_g) * dense_u).astype(jnp.bfloat16)
    dense_out = jnp.dot(
        dense_hidden,
        lax.all_gather(dense_down, "ep", axis=1, tiled=True),
        preferred_element_type=jnp.float32,
    )
    mix = jax.nn.sigmoid(jnp.sum(normed.astype(jnp.float32) * mix_vector, axis=1))
    return mix[:, None] * dense_out


def on_device(
    tokens,
    norm_gain,
    expert_ids,
    gate_weights,
    w_gate,
    w_up,
    w_down,
    dense_gate,
    dense_up,
    dense_down,
    mix_vector,
):
    groups = lax.axis_size("ep")
    ring = lax.axis_size("tp")
    if fits(groups, ring, tokens, w_gate, dense_gate):
        return fused_layer(
            groups, ring, tokens, norm_gain, expert_ids, gate_weights,
            w_gate, w_up, w_down, dense_gate, dense_up, dense_down, mix_vector,
        )
    values = tokens.astype(jnp.float32)
    scale = lax.rsqrt(jnp.mean(values * values, axis=1, keepdims=True) + eps)
    normed = (values * scale * norm_gain).astype(jnp.bfloat16)
    count_tok, topk = expert_ids.shape
    width = tokens.shape[1]
    capacity = 2 * count_tok * topk // groups
    flat_ids = expert_ids.reshape(-1)
    onehot = (flat_ids[:, None] == jnp.arange(groups, dtype=jnp.int32)[None, :]).astype(jnp.int32)
    before = jnp.cumsum(onehot, axis=0) - onehot
    slot = jnp.sum(before * onehot, axis=1)
    dest = flat_ids * capacity + slot
    owner = jnp.arange(count_tok * topk, dtype=jnp.int32) // topk
    buffer = jnp.zeros((groups * capacity, width), jnp.bfloat16).at[dest].set(normed[owner])
    arrived = lax.all_to_all(
        buffer.reshape(groups, capacity, width), "ep", split_axis=0, concat_axis=0, tiled=True
    )
    rows = arrived.reshape(groups * capacity, width)
    gate = jnp.dot(
        rows,
        lax.all_gather(w_gate, "tp", axis=2, tiled=True)[0],
        preferred_element_type=jnp.float32,
    )
    upper = jnp.dot(
        rows, lax.all_gather(w_up, "tp", axis=2, tiled=True)[0], preferred_element_type=jnp.float32
    )
    hidden_all = (jax.nn.silu(gate) * upper).astype(jnp.bfloat16)
    expert_out = lax.dot_general(
        hidden_all,
        lax.all_gather(w_down, "tp", axis=2, tiled=True)[0],
        (((1,), (1,)), ((), ())),
        preferred_element_type=jnp.float32,
    )
    results = expert_out.astype(jnp.bfloat16).reshape(groups, capacity, width)
    returned = lax.all_to_all(results, "ep", split_axis=0, concat_axis=0, tiled=True)
    picked = returned.reshape(groups * capacity, width)[dest].reshape(count_tok, topk, width)
    routed = jnp.einsum("tk,tkd->td", gate_weights, picked.astype(jnp.float32))
    side = dense_branch(normed, dense_gate, dense_up, dense_down, mix_vector)
    return (routed + side).astype(jnp.bfloat16)


def solution(mesh):
    placed = (
        P(("ep", "tp"), None),
        P(),
        P(("ep", "tp"), None),
        P(("ep", "tp"), None),
        P("ep", None, "tp"),
        P("ep", None, "tp"),
        P("ep", None, "tp"),
        P("ep", None),
        P("ep", None),
        P(None, "ep"),
        P(),
    )
    return jax.shard_map(
        on_device, mesh=mesh, in_specs=placed, out_specs=P(("ep", "tp"), None), check_vma=False
    )
```

```python
import functools

import jax
import jax.numpy as jnp
from jax import lax
from jax.experimental import pallas as pl
from jax.experimental.pallas import tpu as pltpu
from jax.sharding import PartitionSpec as P

MESH = pl.DeviceIdType.MESH
VMEM_BYTES = 64000 * 1024
CORES = 2
UNIT = 128
LOOK = 2
BEHIND = 2
TAIL = 256
SUB = 8
eps = 1e-06


def moe_kernel(
    ne, nz, x_hbm, wg_hbm, wu_hbm, wd_hbm, dg_hbm, du_hbm, dd_hbm, ids_hbm, gates_hbm,
    gain_hbm, mixv_hbm, out_ref,
    xin, xg, ws, dgs, dus, dds, gbuf, hbuf, own, keep, ysend, yrecv, relay, side, mix_ref, wts, wcol,
    ids_ref, gates_ref, gain_ref, mixv_ref,
    lsem, wrecv, wright, wleft, wpartner, xsend, xrecv, crecv, precv,
    tsend, trecv, gsem, dsem, drecv, rsend, rrecv,
):
    me = lax.axis_index("ep")
    tp = lax.axis_index("tp")
    z = tp // CORES
    c = tp % CORES
    rows, width = xg.shape[1], xg.shape[2]
    nj = crecv.shape[0]
    half = rows // 2
    shard = ws.shape[4]
    across, along, diagonal = me + 1 - 2 * (me % 2), (me + 2) % ne, ne - 1 - me
    peers = [across, along, diagonal]
    partner = z * CORES + (1 - c)

    local = [pltpu.make_async_copy(wg_hbm, ws.at[z, c, 0], lsem.at[0])]
    local.append(pltpu.make_async_copy(wu_hbm, ws.at[z, c, 1], lsem.at[1]))
    local.append(pltpu.make_async_copy(x_hbm, xin, lsem.at[2]))
    local.append(pltpu.make_async_copy(wd_hbm, ws.at[z, c, 2], lsem.at[3]))
    for p, (ref, slot) in enumerate(((dg_hbm, dgs), (du_hbm, dus), (dd_hbm, dds))):
        local.append(pltpu.make_async_copy(ref, slot.at[0], lsem.at[4 + p]))
    smalls = ((ids_hbm, ids_ref), (gates_hbm, gates_ref), (gain_hbm, gain_ref), (mixv_hbm, mixv_ref))
    for p, (ref, slot) in enumerate(smalls):
        local.append(pltpu.make_async_copy(ref, slot, lsem.at[7 + p]))
    for copy in local:
        copy.start()

    barrier = pltpu.get_barrier_semaphore()
    for peer in (across, along):
        pl.semaphore_signal(barrier, inc=1, device_id={"ep": peer}, device_id_type=MESH)
    pl.semaphore_signal(barrier, inc=1, device_id={"tp": partner}, device_id_type=MESH)

    @pl.when(z > 0)
    def _():
        pl.semaphore_signal(barrier, inc=1, device_id={"tp": tp - CORES}, device_id_type=MESH)

    @pl.when(z < nz - 1)
    def _():
        pl.semaphore_signal(barrier, inc=1, device_id={"tp": tp + CORES}, device_id_type=MESH)

    neighbours = (z + nz - 1) // nz + (2 * nz - 2 - z) // nz
    with jax.named_scope("barrier"):
        pl.semaphore_wait(barrier, 3 + neighbours)

    def remote(src, dst, send, recv, **device):
        return pltpu.make_async_remote_copy(
            src_ref=src, dst_ref=dst, send_sem=send, recv_sem=recv,
            device_id=device, device_id_type=MESH,
        )

    def weight_copy(src, p, target, sems):
        piece = ws.at[src, c, p]
        return remote(piece, piece, sems.at[src], wrecv.at[src, c, p], tp=target)

    def to_right(src, p):
        weight_copy(src, p, tp + CORES, wright).start()

    def to_left(src, p):
        weight_copy(src, p, tp - CORES, wleft).start()

    def to_partner(src, p):
        weight_copy(src, p, partner, wpartner).start()

    def await_piece(src, color, p):
        piece = ws.at[src, color, p]
        remote(piece, piece, wpartner.at[src], wrecv.at[src, color, p], tp=partner).wait_recv()

    def await_sent(src, sems, count):
        piece = ws.at[src, c, :count]
        remote(piece, piece, sems.at[src], wrecv.at[src, c, 0], tp=partner).wait_send()

    def far_main(src, color, target):
        piece = ws.at[src, color, 1] if color else ws.at[src, 0, 1, : width - TAIL]
        return remote(piece, piece, xsend.at[0], wrecv.at[src, color, 1], tp=target)

    def far_tail(src, target):
        piece = ws.at[src, 0, 1, width - TAIL :]
        return remote(piece, piece, xsend.at[1], xrecv.at[0], tp=target)

    def by_color(fn):
        for color in range(CORES):
            pl.when(c == color)(functools.partial(fn, color))

    def at(j, fn):
        if not isinstance(j, int):
            pl.when((j >= 0) & (j < nj))(lambda: fn(j))
        elif 0 <= j < nj:
            fn(j)

    def columns(j):
        return pl.ds(pl.multiple_of(j * UNIT, UNIT), UNIT)

    def chunk_copy(src, j, target, sems, recv):
        piece = ws.at[src, c, 2, columns(j)]
        return remote(piece, piece, sems.at[src], recv, tp=target)

    def order(src, there):
        return (src - there + nz) % nz - 1

    def c_right(src, j):
        chunk_copy(src, j, tp + CORES, wright, crecv.at[j, order(src, z + 1)]).start()

    def c_left(src, j):
        chunk_copy(src, j, tp - CORES, wleft, crecv.at[j, order(src, z - 1)]).start()

    def c_partner(src, j):
        chunk_copy(src, j, partner, wpartner, precv.at[j]).start()

    def arrive(src, j):
        chunk_copy(src, j, partner, wpartner, crecv.at[j, order(src, z)]).wait_recv()
        c_partner(src, j)

    def token_copy(k):
        block = (me, me, across, along)[k]
        peer = (across, along, along, across)[k]
        low, size = ((0, rows), (0, rows), (0, half), (half, half))[k]
        piece = xg.at[block, low : low + size]
        return remote(piece, piece, tsend.at[k], trecv.at[k], ep=peer)

    def await_token(k):
        block = (across, along, diagonal, diagonal)[k]
        low, size = ((0, rows), (0, rows), (0, half), (half, half))[k]
        piece = xg.at[block, low : low + size]
        remote(piece, piece, tsend.at[k], trecv.at[k], ep=across).wait_recv()

    def gate_copy(k):
        return remote(wts.at[0], wts.at[1 + k], gsem.at[0], gsem.at[1 + k], ep=peers[k])

    def gate_all():
        piece = wts.at[1:]
        return remote(piece, piece, gsem.at[0], gsem.at[1], ep=across)

    def await_gate(k):
        piece = wts.at[1 + k]
        remote(piece, piece, gsem.at[0], gsem.at[1 + k], ep=across).wait_recv()

    def dense_piece(p, blocks, color):
        slot = (dgs, dus, dds)[p]
        part = slot.shape[1] // CORES
        return slot.at[blocks, pl.ds(pl.multiple_of(color * part, part), part)]

    def dense_copy(k, p):
        lands = dense_piece(p, 1 + k, c)
        return remote(dense_piece(p, 0, c), lands, dsem.at[p], drecv.at[k, p], ep=peers[k])

    def dense_partner(k, p, color):
        piece = dense_piece(p, 1 + k, color)
        return remote(piece, piece, dsem.at[3 + p], drecv.at[ne - 1 + k, p], tp=partner)

    def dense_sent(p):
        piece = dense_piece(p, pl.ds(1, ne - 1), c)
        for first in (0, 3):
            remote(piece, piece, dsem.at[first + p], drecv.at[0, p], tp=partner).wait_send()

    for p in range(2):
        local[p].wait()

        @pl.when(z < nz - 1)
        def _():
            to_right(z, p)

        @pl.when(z > 0)
        def _():
            to_left(z, p)

        to_partner(z, p)
    for p in (2, 7, 8, 9, 10):
        local[p].wait()

    expert = lax.broadcasted_iota(jnp.int32, (SUB, rows), 0)
    named, gate = ids_ref[...], gates_ref[...]
    weight = jnp.zeros((SUB, rows), jnp.float32)
    for k in range(ids_ref.shape[0]):
        weight += jnp.where(named[k : k + 1, :] == expert, gate[k : k + 1, :], 0.0)
    wts[0] = weight
    tile = 32

    def norm(i, carry):
        at = pl.ds(pl.multiple_of(i * tile, tile), tile)
        v = xin[at, :].astype(jnp.float32)
        scale = lax.rsqrt(jnp.sum(v * v, axis=1, keepdims=True) * (1.0 / width) + eps)
        n = (v * scale * gain_ref[...]).astype(jnp.bfloat16)
        xg[me, at, :] = n
        m = jnp.sum(n.astype(jnp.float32) * mixv_ref[...], axis=1, keepdims=True)
        mix_ref[at, :] = 1.0 / (1.0 + jnp.exp(-m))
        return carry

    with jax.named_scope("norm"):
        lax.fori_loop(0, rows // tile, norm, 0)
    local[3].wait()

    def own_chunks(j, carry):
        c_partner(z, j)

        @pl.when(z == 0)
        def _():
            c_right(z, j)

        @pl.when(z == nz - 1)
        def _():
            c_left(z, j)

        return carry

    lax.fori_loop(0, nj, own_chunks, 0)
    for k in range(2):
        token_copy(k).start()
    for k in range(2):
        gate_copy(k).start()

    def forward(d, p):
        @pl.when(z >= d)
        def _():
            await_piece(z - d, c, p)

            @pl.when(z < nz - 1)
            def _():
                if d == nz - 2 and p == 1:
                    by_color(lambda color: far_main(z - d, color, tp + CORES).start())
                else:
                    to_right(z - d, p)

            to_partner(z - d, p)

        @pl.when(z + d < nz)
        def _():
            await_piece(z + d, c, p)

            @pl.when(z > 0)
            def _():
                if d == nz - 2 and p == 1:
                    by_color(lambda color: far_main(z + d, color, tp - CORES).start())
                else:
                    to_left(z + d, p)

            to_partner(z + d, p)

    def weight_of(src, p):
        return jnp.concatenate([ws[src, i, p] for i in range(CORES)], axis=1)

    def gate_part(src):
        await_piece(src, 1 - c, 0)

        def one(b, carry):
            g = jnp.dot(xg[b], weight_of(src, 0), preferred_element_type=jnp.float32)
            gbuf[b] = g / (1.0 + jnp.exp(-g)) * wcol[b]
            return carry

        lax.fori_loop(0, ne, one, 0)

    def far_forward():
        src = nz - 1 - z

        def one(color):
            far_main(src, color, partner).wait_recv()
            far_main(src, color, partner).start()
            if color:
                far_tail(src, partner).wait_recv()
                far_tail(src, partner).start()

        by_color(one)

    def far_await(src):
        def one(color):
            far_main(src, 1 - color, partner).wait_recv()
            if not color:
                far_tail(src, partner).wait_recv()

        by_color(one)

    def up_part(src, far=False):
        if far:
            far_await(src)
        else:
            await_piece(src, 1 - c, 1)

            @pl.when((c == 1) & (z == 1) & (src == nz - 1))
            def _():
                far_tail(src, tp - CORES).start()

            @pl.when((c == 1) & (z == nz - 2) & (src == 0))
            def _():
                far_tail(src, tp + CORES).start()

        here = pl.ds(pl.multiple_of(src * (CORES * shard), CORES * shard), CORES * shard)

        def one(b, carry):
            u = jnp.dot(xg[b], weight_of(src, 1), preferred_element_type=jnp.float32)
            hbuf[b, :, here] = (gbuf[b] * u).astype(jnp.bfloat16)
            return carry

        lax.fori_loop(0, ne, one, 0)

    def hidden(src):
        gate_part(src)
        up_part(src)

    def both(d, fn):
        @pl.when(z >= d)
        def _():
            fn(z - d)

        @pl.when(z + d < nz)
        def _():
            fn(z + d)

    def ahead(t):
        def one(d, j):
            @pl.when(z == 1)
            def _():
                if d == 0:
                    c_right(z, j)
                elif d == 1:
                    arrive(z - 1, j)
                    c_right(z - 1, j)
                    arrive(z + 1, j)
                else:
                    arrive(z + 2, j)
                    for src in range(nz - 1):
                        c_left(z + src, j)

            @pl.when(z == 2)
            def _():
                if d == 0:
                    c_left(z, j)
                elif d == 1:
                    arrive(z + 1, j)
                    c_left(z + 1, j)
                    arrive(z - 1, j)
                else:
                    arrive(z - 2, j)
                    for src in range(nz - 1):
                        c_right(z - src, j)

        for d in range(nz - 1):
            at(t + LOOK * (nz - 1 - d), functools.partial(one, d))

    for p in range(2):
        with jax.named_scope(f"forward1_{p}"):
            forward(1, p)
    with jax.named_scope("token_relay"):
        for k in range(2):
            await_token(k)
            token_copy(2 + k).start()
    gate_copy(2).start()
    for p in range(3):
        local[4 + p].wait()
        for k in range(ne - 1):
            dense_copy(k, p).start()
    for d in range(2, nz - 1):
        for p in range(2):
            with jax.named_scope(f"forward{d}_{p}"):
                forward(d, p)
    for t in range(LOOK):
        ahead(t - LOOK * (nz - 1))
    with jax.named_scope("gate_wait"):
        for k in range(ne - 1):
            await_gate(k)
    lane = lax.broadcasted_iota(jnp.int32, (rows, SUB), 1)
    for r, b in enumerate([me] + peers):
        column = jnp.where(lane == me, wts[r].T, 0.0)
        wcol[b] = jnp.sum(column, axis=1, keepdims=True)
    with jax.named_scope("token_wait"):
        for k in range(2, 4):
            await_token(k)
    with jax.named_scope("hidden_own"):
        hidden(z)
    for d in range(1, nz - 1):
        with jax.named_scope(f"hidden{d}"):
            both(d, hidden)
        with jax.named_scope(f"ahead{d}"):
            for t in range(LOOK):
                ahead(t - LOOK * (nz - 1 - d))
    with jax.named_scope("dense_wait"):
        for p in range(3):
            for k in range(ne - 1):
                dense_copy(k, p).wait_recv()
                dense_partner(k, p, c).start()
    with jax.named_scope("forward_last0"):
        forward(nz - 1, 0)
    with jax.named_scope("gate_last"):
        both(nz - 1, gate_part)
    with jax.named_scope("dense_partner"):
        for p in range(3):
            for k in range(ne - 1):
                dense_partner(k, p, 1 - c).wait_recv()
    with jax.named_scope("dense_side"):
        dense_side([me] + peers, me, xg, dgs, dus, dds, mix_ref, side)
    with jax.named_scope("forward_last1"):
        pl.when((z == 0) | (z == nz - 1))(far_forward)
    with jax.named_scope("up_last"):
        both(nz - 1, functools.partial(up_part, far=True))

    def back(k, j):
        block = (diagonal, diagonal, across, along, along, across)[k]
        peer = (across, along, across, along, along, across)[k]
        spot = (0, 1, 0, 1, 1, 0)[k]
        lands = relay.at[k, j] if k < 2 else yrecv.at[spot, k % 2, j]
        return remote(ysend.at[block, k % 2, j], lands, rsend.at[0], rrecv.at[j, min(k // 2, 1)], ep=peer)

    def take(j):
        ahead(j)

        @pl.when(z == 0)
        def _():
            for d in range(1, nz):
                arrive(d, j)

        @pl.when(z == nz - 1)
        def _():
            for d in range(1, nz):
                arrive(z - d, j)

        piece = ws.at[:, 1 - c, 2, columns(j)]
        remote(piece, piece, wpartner.at[0], precv.at[j], tp=partner).wait_recv()

    def produce(j):
        here = columns(j)
        w = jnp.concatenate([ws[s, i, 2, here, :] for s in range(nz) for i in range(CORES)], axis=1)
        blocks = (diagonal, across, along, me)
        full = lax.dot_general(
            jnp.concatenate([hbuf[b] for b in blocks], axis=0), w,
            (((1,), (1,)), ((), ())), preferred_element_type=jnp.float32,
        )
        y = [full[i * half : (i + 1) * half] for i in range(2 * ne)]
        for k, i in enumerate((0, 1, 2, 5)):
            ysend[blocks[i // 2], i % 2, j] = y[i].astype(jnp.bfloat16)
            back(k, j).start()
        keep[0, j] = y[4]
        keep[1, j] = y[3]
        own[:, here] = full[(ne - 1) * rows :]

    def pass_on(j):
        piece = relay.at[:, j]
        remote(piece, piece, rsend.at[0], rrecv.at[j, 0], ep=across).wait_recv()
        for k, block in enumerate((along, across)):
            v = keep[k, j] + relay[k, j].astype(jnp.float32)
            ysend[block, k, j] = v.astype(jnp.bfloat16)
            back(4 + k, j).start()

    def combine(j):
        piece = yrecv.at[:, :, j]
        remote(piece, piece, rsend.at[0], rrecv.at[j, 1], ep=across).wait_recv()
        here = columns(j)
        for h in range(2):
            low = h * half
            total = side[low : low + half, here] + own[low : low + half, here]
            for k in range(2):
                total = total + yrecv[k, h, j].astype(jnp.float32)
            out_ref[low : low + half, here] = total.astype(jnp.bfloat16)

    def step(j, carry):
        with jax.named_scope("take"):
            take(j)
        with jax.named_scope("produce"):
            produce(j)
        with jax.named_scope("pass_on"):
            at(j - BEHIND, pass_on)
        with jax.named_scope("combine"):
            pl.when(j < nj - 2)(lambda: at(j - 2 * BEHIND, combine))
        return carry

    lax.fori_loop(0, nj, step, 0)

    def pass_rest(j, carry):
        pass_on(j)
        return carry

    def combine_rest(j, carry):
        combine(j)
        return carry

    with jax.named_scope("pass_rest"):
        lax.fori_loop(nj - BEHIND, nj, pass_rest, 0)
    with jax.named_scope("combine_rest"):
        lax.fori_loop(nj - 2 * BEHIND - 2, nj, combine_rest, 0)

    drain = jax.named_scope("drain")
    drain.__enter__()
    for k in range(4):
        token_copy(k).wait_send()
    gate_all().wait_send()
    for p in range(3):
        dense_sent(p)
    for src in range(nz):
        for sems, there, far in (
            (wright, (z < nz - 1) & (z >= src), (z == nz - 2) & (src == 0)),
            (wleft, (z > 0) & (z <= src), (z == 1) & (src == nz - 1)),
            (wpartner, z >= 0, (z == nz - 1 - src) & (src % (nz - 1) == 0)),
        ):
            pl.when(there & far)(functools.partial(await_sent, src, sems, 2))
            pl.when(there & jnp.logical_not(far))(functools.partial(await_sent, src, sems, 3))

    def far_sent(color):
        far_main(0, color, partner).wait_send()
        if color:
            far_tail(0, partner).wait_send()

    by_color(far_sent)
    piece = ysend.at[: ne - 1]
    remote(piece, piece, rsend.at[0], rrecv.at[0, 0], ep=across).wait_send()
    drain.__exit__(None, None, None)


def dense_side(owners, me, xg, dgs, dus, dds, mix_ref, side):
    deep, wide = dgs.shape[1], dds.shape[2]
    g = u = None
    for r, e in enumerate(owners):
        x = xg[me, :, pl.ds(pl.multiple_of(e * deep, deep), deep)]
        ge = jnp.dot(x, dgs[r], preferred_element_type=jnp.float32)
        ue = jnp.dot(x, dus[r], preferred_element_type=jnp.float32)
        g, u = (ge, ue) if r == 0 else (g + ge, u + ue)
    h = (g / (1.0 + jnp.exp(-g)) * u).astype(jnp.bfloat16)
    for r, e in enumerate(owners):
        o = jnp.dot(h, dds[r], preferred_element_type=jnp.float32)
        side[:, pl.ds(pl.multiple_of(e * wide, wide), wide)] = mix_ref[...] * o


def fused_layer(
    ne, tp, tokens, norm_gain, expert_ids, gate_weights,
    w_gate, w_up, w_down, dense_gate, dense_up, dense_down, mix_vector,
):
    nz = tp // CORES
    rows, width = tokens.shape
    topk = expert_ids.shape[1]
    shard = w_gate.shape[2]
    nj = width // UNIT
    half = rows // 2
    bf, f32 = jnp.bfloat16, jnp.float32
    dma = pltpu.SemaphoreType.DMA
    hbm = pl.BlockSpec(memory_space=pl.ANY)
    vmem = pl.BlockSpec(memory_space=pltpu.VMEM)
    flops = 6 * ne * rows * width * shard * tp
    return pl.pallas_call(
        functools.partial(moe_kernel, ne, nz),
        out_shape=pltpu.VMEM((rows, width), bf),
        in_specs=[hbm] * 11,
        out_specs=vmem,
        scratch_shapes=[
            pltpu.VMEM((rows, width), bf),
            pltpu.VMEM((ne, rows, width), bf),
            pltpu.VMEM((nz, CORES, 3, width, shard), bf),
            pltpu.VMEM((ne,) + dense_gate.shape, bf),
            pltpu.VMEM((ne,) + dense_up.shape, bf),
            pltpu.VMEM((ne,) + dense_down.shape, bf),
            pltpu.VMEM((ne, rows, CORES * shard), f32),
            pltpu.VMEM((ne, rows, tp * shard), bf),
            pltpu.VMEM((rows, width), f32),
            pltpu.VMEM((2, nj, half, UNIT), f32),
            pltpu.VMEM((ne, 2, nj, half, UNIT), bf),
            pltpu.VMEM((2, 2, nj, half, UNIT), bf),
            pltpu.VMEM((2, nj, half, UNIT), bf),
            pltpu.VMEM((rows, width), f32),
            pltpu.VMEM((rows, 1), f32),
            pltpu.VMEM((ne, SUB, rows), f32),
            pltpu.VMEM((ne, rows, 1), f32),
            pltpu.VMEM((topk, rows), jnp.int32),
            pltpu.VMEM((topk, rows), f32),
            pltpu.VMEM((1, width), f32),
            pltpu.VMEM((1, width), f32),
            dma((11,)),
            dma((nz, CORES, 2)),
            dma((nz,)),
            dma((nz,)),
            dma((nz,)),
            dma((2,)),
            dma((1,)),
            dma((nj, nz - 1)),
            dma((nj,)),
            dma((4,)),
            dma((4,)),
            dma((ne,)),
            dma((6,)),
            dma((2 * ne - 2, 3)),
            dma((1,)),
            dma((nj, 2)),
        ],
        compiler_params=pltpu.CompilerParams(
            collective_id=0, has_side_effects=True, vmem_limit_bytes=VMEM_BYTES
        ),
        cost_estimate=pl.CostEstimate(
            flops=flops, bytes_accessed=8 * rows * width, transcendentals=ne * rows * shard * tp
        ),
    )(
        tokens, w_gate[0], w_up[0], w_down[0], dense_gate, dense_up, dense_down,
        expert_ids.T, gate_weights.T, norm_gain.reshape(1, width), mix_vector.reshape(1, width),
    )


def fits(ne, tp, tokens, w_gate, dense_gate):
    rows, width = tokens.shape
    shard = w_gate.shape[2]
    block = rows * width
    size = 2 * ne * block * 2 + 24 * block + 6 * width * shard * tp
    size += 2 * ne * rows * shard * tp + 6 * ne * dense_gate.size + 1024 * ne * rows
    size += 8 * ne * rows * shard
    aligned = shard % 128 == 0 and width % (8 * UNIT) == 0 and width > TAIL and rows % 64 == 0
    return ne == 4 and tp == 4 * CORES and aligned and size < VMEM_BYTES * 15 // 16


def dense_branch(normed, dense_gate, dense_up, dense_down, mix_vector):
    dense_g = jnp.dot(
        normed,
        lax.all_gather(dense_gate, "ep", axis=0, tiled=True),
        preferred_element_type=jnp.float32,
    )
    dense_u = jnp.dot(
        normed,
        lax.all_gather(dense_up, "ep", axis=0, tiled=True),
        preferred_element_type=jnp.float32,
    )
    dense_hidden = (jax.nn.silu(dense_g) * dense_u).astype(jnp.bfloat16)
    dense_out = jnp.dot(
        dense_hidden,
        lax.all_gather(dense_down, "ep", axis=1, tiled=True),
        preferred_element_type=jnp.float32,
    )
    mix = jax.nn.sigmoid(jnp.sum(normed.astype(jnp.float32) * mix_vector, axis=1))
    return mix[:, None] * dense_out


def on_device(
    tokens,
    norm_gain,
    expert_ids,
    gate_weights,
    w_gate,
    w_up,
    w_down,
    dense_gate,
    dense_up,
    dense_down,
    mix_vector,
):
    groups = lax.axis_size("ep")
    ring = lax.axis_size("tp")
    if fits(groups, ring, tokens, w_gate, dense_gate):
        return fused_layer(
            groups, ring, tokens, norm_gain, expert_ids, gate_weights,
            w_gate, w_up, w_down, dense_gate, dense_up, dense_down, mix_vector,
        )
    values = tokens.astype(jnp.float32)
    scale = lax.rsqrt(jnp.mean(values * values, axis=1, keepdims=True) + eps)
    normed = (values * scale * norm_gain).astype(jnp.bfloat16)
    count_tok, topk = expert_ids.shape
    width = tokens.shape[1]
    capacity = 2 * count_tok * topk // groups
    flat_ids = expert_ids.reshape(-1)
    onehot = (flat_ids[:, None] == jnp.arange(groups, dtype=jnp.int32)[None, :]).astype(jnp.int32)
    before = jnp.cumsum(onehot, axis=0) - onehot
    slot = jnp.sum(before * onehot, axis=1)
    dest = flat_ids * capacity + slot
    owner = jnp.arange(count_tok * topk, dtype=jnp.int32) // topk
    buffer = jnp.zeros((groups * capacity, width), jnp.bfloat16).at[dest].set(normed[owner])
    arrived = lax.all_to_all(
        buffer.reshape(groups, capacity, width), "ep", split_axis=0, concat_axis=0, tiled=True
    )
    rows = arrived.reshape(groups * capacity, width)
    gate = jnp.dot(
        rows,
        lax.all_gather(w_gate, "tp", axis=2, tiled=True)[0],
        preferred_element_type=jnp.float32,
    )
    upper = jnp.dot(
        rows, lax.all_gather(w_up, "tp", axis=2, tiled=True)[0], preferred_element_type=jnp.float32
    )
    hidden_all = (jax.nn.silu(gate) * upper).astype(jnp.bfloat16)
    expert_out = lax.dot_general(
        hidden_all,
        lax.all_gather(w_down, "tp", axis=2, tiled=True)[0],
        (((1,), (1,)), ((), ())),
        preferred_element_type=jnp.float32,
    )
    results = expert_out.astype(jnp.bfloat16).reshape(groups, capacity, width)
    returned = lax.all_to_all(results, "ep", split_axis=0, concat_axis=0, tiled=True)
    picked = returned.reshape(groups * capacity, width)[dest].reshape(count_tok, topk, width)
    routed = jnp.einsum("tk,tkd->td", gate_weights, picked.astype(jnp.float32))
    side = dense_branch(normed, dense_gate, dense_up, dense_down, mix_vector)
    return (routed + side).astype(jnp.bfloat16)


def solution(mesh):
    placed = (
        P(("ep", "tp"), None),
        P(),
        P(("ep", "tp"), None),
        P(("ep", "tp"), None),
        P("ep", None, "tp"),
        P("ep", None, "tp"),
        P("ep", None, "tp"),
        P("ep", None),
        P("ep", None),
        P(None, "ep"),
        P(),
    )
    return jax.shard_map(
        on_device, mesh=mesh, in_specs=placed, out_specs=P(("ep", "tp"), None), check_vma=False
    )
```

```python
import functools

import jax
import jax.numpy as jnp
from jax import lax
from jax.experimental import pallas as pl
from jax.experimental.pallas import tpu as pltpu
from jax.sharding import PartitionSpec as P

MESH = pl.DeviceIdType.MESH
VMEM_BYTES = 64000 * 1024
CORES = 2
UNIT = 128
LOOK = 2
BEHIND = 2
TAIL = 256
SUB = 8
eps = 1e-06


def moe_kernel(
    ne, nz, x_hbm, wg_hbm, wu_hbm, wd_hbm, dg_hbm, du_hbm, dd_hbm, ids_hbm, gates_hbm,
    gain_hbm, mixv_hbm, out_ref,
    xin, xg, ws, dgs, dus, dds, gbuf, hbuf, own, keep, ysend, yrecv, relay, side, mix_ref, wts, wcol,
    ids_ref, gates_ref, gain_ref, mixv_ref,
    lsem, wrecv, wright, wleft, wpartner, xsend, xrecv, crecv, precv,
    tsend, trecv, gsem, dsem, drecv, rsend, rrecv,
):
    me = lax.axis_index("ep")
    tp = lax.axis_index("tp")
    z = tp // CORES
    c = tp % CORES
    rows, width = xg.shape[1], xg.shape[2]
    nj = crecv.shape[0]
    half = rows // 2
    shard = ws.shape[4]
    across, along, diagonal = me + 1 - 2 * (me % 2), (me + 2) % ne, ne - 1 - me
    peers = [across, along, diagonal]
    partner = z * CORES + (1 - c)

    local = [pltpu.make_async_copy(wg_hbm, ws.at[z, c, 0], lsem.at[0])]
    local.append(pltpu.make_async_copy(wu_hbm, ws.at[z, c, 1], lsem.at[1]))
    local.append(pltpu.make_async_copy(x_hbm, xin, lsem.at[2]))
    local.append(pltpu.make_async_copy(wd_hbm, ws.at[z, c, 2], lsem.at[3]))
    for p, (ref, slot) in enumerate(((dg_hbm, dgs), (du_hbm, dus), (dd_hbm, dds))):
        local.append(pltpu.make_async_copy(ref, slot.at[0], lsem.at[4 + p]))
    smalls = ((ids_hbm, ids_ref), (gates_hbm, gates_ref), (gain_hbm, gain_ref), (mixv_hbm, mixv_ref))
    for p, (ref, slot) in enumerate(smalls):
        local.append(pltpu.make_async_copy(ref, slot, lsem.at[7 + p]))
    for copy in local:
        copy.start()

    barrier = pltpu.get_barrier_semaphore()
    for peer in (across, along):
        pl.semaphore_signal(barrier, inc=1, device_id={"ep": peer}, device_id_type=MESH)
    pl.semaphore_signal(barrier, inc=1, device_id={"tp": partner}, device_id_type=MESH)

    @pl.when(z > 0)
    def _():
        pl.semaphore_signal(barrier, inc=1, device_id={"tp": tp - CORES}, device_id_type=MESH)

    @pl.when(z < nz - 1)
    def _():
        pl.semaphore_signal(barrier, inc=1, device_id={"tp": tp + CORES}, device_id_type=MESH)

    neighbours = (z + nz - 1) // nz + (2 * nz - 2 - z) // nz
    with jax.named_scope("barrier"):
        pl.semaphore_wait(barrier, 3 + neighbours)

    def remote(src, dst, send, recv, **device):
        return pltpu.make_async_remote_copy(
            src_ref=src, dst_ref=dst, send_sem=send, recv_sem=recv,
            device_id=device, device_id_type=MESH,
        )

    def weight_copy(src, p, target, sems):
        piece = ws.at[src, c, p]
        return remote(piece, piece, sems.at[src], wrecv.at[src, c, p], tp=target)

    def to_right(src, p):
        weight_copy(src, p, tp + CORES, wright).start()

    def to_left(src, p):
        weight_copy(src, p, tp - CORES, wleft).start()

    def to_partner(src, p):
        weight_copy(src, p, partner, wpartner).start()

    def await_piece(src, color, p):
        piece = ws.at[src, color, p]
        remote(piece, piece, wpartner.at[src], wrecv.at[src, color, p], tp=partner).wait_recv()

    def await_sent(src, sems, count):
        piece = ws.at[src, c, :count]
        remote(piece, piece, sems.at[src], wrecv.at[src, c, 0], tp=partner).wait_send()

    def far_main(src, color, target):
        piece = ws.at[src, color, 1] if color else ws.at[src, 0, 1, : width - TAIL]
        return remote(piece, piece, xsend.at[0], wrecv.at[src, color, 1], tp=target)

    def far_tail(src, target):
        piece = ws.at[src, 0, 1, width - TAIL :]
        return remote(piece, piece, xsend.at[1], xrecv.at[0], tp=target)

    def by_color(fn):
        for color in range(CORES):
            pl.when(c == color)(functools.partial(fn, color))

    def at(j, fn):
        if not isinstance(j, int):
            pl.when((j >= 0) & (j < nj))(lambda: fn(j))
        elif 0 <= j < nj:
            fn(j)

    def columns(j):
        return pl.ds(pl.multiple_of(j * UNIT, UNIT), UNIT)

    def chunk_copy(src, j, target, sems, recv):
        piece = ws.at[src, c, 2, columns(j)]
        return remote(piece, piece, sems.at[src], recv, tp=target)

    def order(src, there):
        return (src - there + nz) % nz - 1

    def c_right(src, j):
        chunk_copy(src, j, tp + CORES, wright, crecv.at[j, order(src, z + 1)]).start()

    def c_left(src, j):
        chunk_copy(src, j, tp - CORES, wleft, crecv.at[j, order(src, z - 1)]).start()

    def c_partner(src, j):
        chunk_copy(src, j, partner, wpartner, precv.at[j]).start()

    def arrive(src, j):
        chunk_copy(src, j, partner, wpartner, crecv.at[j, order(src, z)]).wait_recv()
        c_partner(src, j)

    def token_copy(k):
        block = (me, me, across, along)[k]
        peer = (across, along, along, across)[k]
        low, size = ((0, rows), (0, rows), (0, half), (half, half))[k]
        piece = xg.at[block, low : low + size]
        return remote(piece, piece, tsend.at[0], trecv.at[k], ep=peer)

    def await_token(k):
        block = (across, along, diagonal, diagonal)[k]
        low, size = ((0, rows), (0, rows), (0, half), (half, half))[k]
        piece = xg.at[block, low : low + size]
        remote(piece, piece, tsend.at[0], trecv.at[k], ep=across).wait_recv()

    def gate_copy(k):
        return remote(wts.at[0], wts.at[1 + k], gsem.at[0], gsem.at[1 + k], ep=peers[k])

    def gate_all():
        piece = wts.at[1:]
        return remote(piece, piece, gsem.at[0], gsem.at[1], ep=across)

    def await_gate(k):
        piece = wts.at[1 + k]
        remote(piece, piece, gsem.at[0], gsem.at[1 + k], ep=across).wait_recv()

    def dense_piece(p, blocks, color):
        slot = (dgs, dus, dds)[p]
        part = slot.shape[1] // CORES
        return slot.at[blocks, pl.ds(pl.multiple_of(color * part, part), part)]

    def dense_copy(k, p):
        lands = dense_piece(p, 1 + k, c)
        return remote(dense_piece(p, 0, c), lands, dsem.at[p], drecv.at[0, p], ep=peers[k])

    def dense_partner(k, p):
        piece = dense_piece(p, 1 + k, c)
        return remote(piece, piece, dsem.at[3 + p], drecv.at[1, p], tp=partner)

    def dense_all(p, i, color):
        piece = dense_piece(p, pl.ds(1, ne - 1), color)
        return remote(piece, piece, dsem.at[3 * i + p], drecv.at[i, p], tp=partner)

    for p in range(2):
        local[p].wait()

        @pl.when(z < nz - 1)
        def _():
            to_right(z, p)

        @pl.when(z > 0)
        def _():
            to_left(z, p)

        to_partner(z, p)
    for p in (2, 7, 8, 9, 10):
        local[p].wait()

    expert = lax.broadcasted_iota(jnp.int32, (SUB, rows), 0)
    named, gate = ids_ref[...], gates_ref[...]
    weight = jnp.zeros((SUB, rows), jnp.float32)
    for k in range(ids_ref.shape[0]):
        weight += jnp.where(named[k : k + 1, :] == expert, gate[k : k + 1, :], 0.0)
    wts[0] = weight
    tile = 32

    def norm(i, carry):
        at = pl.ds(pl.multiple_of(i * tile, tile), tile)
        v = xin[at, :].astype(jnp.float32)
        scale = lax.rsqrt(jnp.sum(v * v, axis=1, keepdims=True) * (1.0 / width) + eps)
        n = (v * scale * gain_ref[...]).astype(jnp.bfloat16)
        xg[me, at, :] = n
        m = jnp.sum(n.astype(jnp.float32) * mixv_ref[...], axis=1, keepdims=True)
        mix_ref[at, :] = 1.0 / (1.0 + jnp.exp(-m))
        return carry

    with jax.named_scope("norm"):
        lax.fori_loop(0, rows // tile, norm, 0)
    local[3].wait()

    def own_chunks(j, carry):
        c_partner(z, j)

        @pl.when(z == 0)
        def _():
            c_right(z, j)

        @pl.when(z == nz - 1)
        def _():
            c_left(z, j)

        return carry

    lax.fori_loop(0, nj, own_chunks, 0)
    for k in range(2):
        token_copy(k).start()
    for k in range(2):
        gate_copy(k).start()

    def forward(d, p):
        @pl.when(z >= d)
        def _():
            await_piece(z - d, c, p)

            @pl.when(z < nz - 1)
            def _():
                if d == nz - 2 and p == 1:
                    by_color(lambda color: far_main(z - d, color, tp + CORES).start())
                else:
                    to_right(z - d, p)

            to_partner(z - d, p)

        @pl.when(z + d < nz)
        def _():
            await_piece(z + d, c, p)

            @pl.when(z > 0)
            def _():
                if d == nz - 2 and p == 1:
                    by_color(lambda color: far_main(z + d, color, tp - CORES).start())
                else:
                    to_left(z + d, p)

            to_partner(z + d, p)

    def weight_of(src, p):
        return jnp.concatenate([ws[src, i, p] for i in range(CORES)], axis=1)

    def gate_part(src):
        await_piece(src, 1 - c, 0)

        def one(b, carry):
            g = jnp.dot(xg[b], weight_of(src, 0), preferred_element_type=jnp.float32)
            gbuf[b] = g / (1.0 + jnp.exp(-g)) * wcol[b]
            return carry

        lax.fori_loop(0, ne, one, 0)

    def far_forward():
        src = nz - 1 - z

        def one(color):
            far_main(src, color, partner).wait_recv()
            far_main(src, color, partner).start()
            if color:
                far_tail(src, partner).wait_recv()
                far_tail(src, partner).start()

        by_color(one)

    def far_await(src):
        def one(color):
            far_main(src, 1 - color, partner).wait_recv()
            if not color:
                far_tail(src, partner).wait_recv()

        by_color(one)

    def up_part(src, far=False):
        if far:
            far_await(src)
        else:
            await_piece(src, 1 - c, 1)

            @pl.when((c == 1) & (z == 1) & (src == nz - 1))
            def _():
                far_tail(src, tp - CORES).start()

            @pl.when((c == 1) & (z == nz - 2) & (src == 0))
            def _():
                far_tail(src, tp + CORES).start()

        here = pl.ds(pl.multiple_of(src * (CORES * shard), CORES * shard), CORES * shard)

        def one(b, carry):
            u = jnp.dot(xg[b], weight_of(src, 1), preferred_element_type=jnp.float32)
            hbuf[b, :, here] = (gbuf[b] * u).astype(jnp.bfloat16)
            return carry

        lax.fori_loop(0, ne, one, 0)

    def hidden(src):
        gate_part(src)
        up_part(src)

    def both(d, fn):
        @pl.when(z >= d)
        def _():
            fn(z - d)

        @pl.when(z + d < nz)
        def _():
            fn(z + d)

    def ahead(t):
        def one(d, j):
            @pl.when(z == 1)
            def _():
                if d == 0:
                    c_right(z, j)
                elif d == 1:
                    arrive(z - 1, j)
                    c_right(z - 1, j)
                    arrive(z + 1, j)
                else:
                    arrive(z + 2, j)
                    for src in range(nz - 1):
                        c_left(z + src, j)

            @pl.when(z == 2)
            def _():
                if d == 0:
                    c_left(z, j)
                elif d == 1:
                    arrive(z + 1, j)
                    c_left(z + 1, j)
                    arrive(z - 1, j)
                else:
                    arrive(z - 2, j)
                    for src in range(nz - 1):
                        c_right(z - src, j)

        for d in range(nz - 1):
            at(t + LOOK * (nz - 1 - d), functools.partial(one, d))

    for p in range(2):
        with jax.named_scope(f"forward1_{p}"):
            forward(1, p)
    with jax.named_scope("token_relay"):
        for k in range(2):
            await_token(k)
            token_copy(2 + k).start()
    gate_copy(2).start()
    for p in range(3):
        local[4 + p].wait()
        for k in range(ne - 1):
            dense_copy(k, p).start()
    for d in range(2, nz - 1):
        for p in range(2):
            with jax.named_scope(f"forward{d}_{p}"):
                forward(d, p)
    for t in range(LOOK):
        ahead(t - LOOK * (nz - 1))
    with jax.named_scope("gate_wait"):
        for k in range(ne - 1):
            await_gate(k)
    lane = lax.broadcasted_iota(jnp.int32, (rows, SUB), 1)
    for r, b in enumerate([me] + peers):
        column = jnp.where(lane == me, wts[r].T, 0.0)
        wcol[b] = jnp.sum(column, axis=1, keepdims=True)
    with jax.named_scope("token_wait"):
        for k in range(2, 4):
            await_token(k)
    with jax.named_scope("hidden_own"):
        hidden(z)
    for d in range(1, nz - 1):
        with jax.named_scope(f"hidden{d}"):
            both(d, hidden)
        with jax.named_scope(f"ahead{d}"):
            for t in range(LOOK):
                ahead(t - LOOK * (nz - 1 - d))
    with jax.named_scope("dense_wait"):
        for p in range(3):
            dense_all(p, 0, c).wait_recv()
            for k in range(ne - 1):
                dense_partner(k, p).start()
    with jax.named_scope("forward_last0"):
        forward(nz - 1, 0)
    with jax.named_scope("gate_last"):
        both(nz - 1, gate_part)
    with jax.named_scope("dense_partner"):
        for p in range(3):
            dense_all(p, 1, 1 - c).wait_recv()
    with jax.named_scope("dense_side"):
        dense_side([me] + peers, me, xg, dgs, dus, dds, mix_ref, side)
    with jax.named_scope("forward_last1"):
        pl.when((z == 0) | (z == nz - 1))(far_forward)
    with jax.named_scope("up_last"):
        both(nz - 1, functools.partial(up_part, far=True))

    def back(k, j):
        block = (diagonal, diagonal, across, along, along, across)[k]
        peer = (across, along, across, along, along, across)[k]
        spot = (0, 1, 0, 1, 1, 0)[k]
        lands = relay.at[k, j] if k < 2 else yrecv.at[spot, k % 2, j]
        return remote(ysend.at[block, k % 2, j], lands, rsend.at[0], rrecv.at[j, min(k // 2, 1)], ep=peer)

    def take(j):
        ahead(j)

        @pl.when(z == 0)
        def _():
            for d in range(1, nz):
                arrive(d, j)

        @pl.when(z == nz - 1)
        def _():
            for d in range(1, nz):
                arrive(z - d, j)

        piece = ws.at[:, 1 - c, 2, columns(j)]
        remote(piece, piece, wpartner.at[0], precv.at[j], tp=partner).wait_recv()

    def produce(j):
        here = columns(j)
        w = jnp.concatenate([ws[s, i, 2, here, :] for s in range(nz) for i in range(CORES)], axis=1)
        blocks = (diagonal, across, along, me)
        full = lax.dot_general(
            jnp.concatenate([hbuf[b] for b in blocks], axis=0), w,
            (((1,), (1,)), ((), ())), preferred_element_type=jnp.float32,
        )
        y = [full[i * half : (i + 1) * half] for i in range(2 * ne)]
        for k, i in enumerate((0, 1, 2, 5)):
            ysend[blocks[i // 2], i % 2, j] = y[i].astype(jnp.bfloat16)
            back(k, j).start()
        keep[0, j] = y[4]
        keep[1, j] = y[3]
        own[:, here] = full[(ne - 1) * rows :]

    def pass_on(j):
        piece = relay.at[:, j]
        remote(piece, piece, rsend.at[0], rrecv.at[j, 0], ep=across).wait_recv()
        for k, block in enumerate((along, across)):
            v = keep[k, j] + relay[k, j].astype(jnp.float32)
            ysend[block, k, j] = v.astype(jnp.bfloat16)
            back(4 + k, j).start()

    def combine(j):
        piece = yrecv.at[:, :, j]
        remote(piece, piece, rsend.at[0], rrecv.at[j, 1], ep=across).wait_recv()
        here = columns(j)
        for h in range(2):
            low = h * half
            total = side[low : low + half, here] + own[low : low + half, here]
            for k in range(2):
                total = total + yrecv[k, h, j].astype(jnp.float32)
            out_ref[low : low + half, here] = total.astype(jnp.bfloat16)

    def step(j, carry):
        with jax.named_scope("take"):
            take(j)
        with jax.named_scope("pass_on"):
            pl.when(j < nj - 1)(lambda: at(j - BEHIND, pass_on))
        with jax.named_scope("produce"):
            produce(j)
        with jax.named_scope("combine"):
            pl.when(j < nj - 2)(lambda: at(j - 2 * BEHIND, combine))
        return carry

    lax.fori_loop(0, nj, step, 0)

    def pass_rest(j, carry):
        pass_on(j)
        return carry

    def combine_rest(j, carry):
        combine(j)
        return carry

    with jax.named_scope("pass_rest"):
        lax.fori_loop(nj - 1 - BEHIND, nj, pass_rest, 0)
    with jax.named_scope("combine_rest"):
        lax.fori_loop(nj - 2 * BEHIND - 2, nj, combine_rest, 0)

    drain = jax.named_scope("drain")
    drain.__enter__()
    piece = xg.at[: ne - 1]
    remote(piece, piece, tsend.at[0], trecv.at[0], ep=across).wait_send()
    gate_all().wait_send()
    for p in range(3):
        for i in range(2):
            dense_all(p, i, c).wait_send()
    for src in range(nz):
        for sems, there, far in (
            (wright, (z < nz - 1) & (z >= src), (z == nz - 2) & (src == 0)),
            (wleft, (z > 0) & (z <= src), (z == 1) & (src == nz - 1)),
            (wpartner, z >= 0, (z == nz - 1 - src) & (src % (nz - 1) == 0)),
        ):
            pl.when(there & far)(functools.partial(await_sent, src, sems, 2))
            pl.when(there & jnp.logical_not(far))(functools.partial(await_sent, src, sems, 3))

    def far_sent(color):
        far_main(0, color, partner).wait_send()
        if color:
            far_tail(0, partner).wait_send()

    by_color(far_sent)
    piece = ysend.at[: ne - 1]
    remote(piece, piece, rsend.at[0], rrecv.at[0, 0], ep=across).wait_send()
    drain.__exit__(None, None, None)


def dense_side(owners, me, xg, dgs, dus, dds, mix_ref, side):
    deep, wide = dgs.shape[1], dds.shape[2]
    g = u = None
    for r, e in enumerate(owners):
        x = xg[me, :, pl.ds(pl.multiple_of(e * deep, deep), deep)]
        ge = jnp.dot(x, dgs[r], preferred_element_type=jnp.float32)
        ue = jnp.dot(x, dus[r], preferred_element_type=jnp.float32)
        g, u = (ge, ue) if r == 0 else (g + ge, u + ue)
    h = (g / (1.0 + jnp.exp(-g)) * u).astype(jnp.bfloat16)
    for r, e in enumerate(owners):
        o = jnp.dot(h, dds[r], preferred_element_type=jnp.float32)
        side[:, pl.ds(pl.multiple_of(e * wide, wide), wide)] = mix_ref[...] * o


def fused_layer(
    ne, tp, tokens, norm_gain, expert_ids, gate_weights,
    w_gate, w_up, w_down, dense_gate, dense_up, dense_down, mix_vector,
):
    nz = tp // CORES
    rows, width = tokens.shape
    topk = expert_ids.shape[1]
    shard = w_gate.shape[2]
    nj = width // UNIT
    half = rows // 2
    bf, f32 = jnp.bfloat16, jnp.float32
    dma = pltpu.SemaphoreType.DMA
    hbm = pl.BlockSpec(memory_space=pl.ANY)
    vmem = pl.BlockSpec(memory_space=pltpu.VMEM)
    flops = 6 * ne * rows * width * shard * tp
    return pl.pallas_call(
        functools.partial(moe_kernel, ne, nz),
        out_shape=pltpu.VMEM((rows, width), bf),
        in_specs=[hbm] * 11,
        out_specs=vmem,
        scratch_shapes=[
            pltpu.VMEM((rows, width), bf),
            pltpu.VMEM((ne, rows, width), bf),
            pltpu.VMEM((nz, CORES, 3, width, shard), bf),
            pltpu.VMEM((ne,) + dense_gate.shape, bf),
            pltpu.VMEM((ne,) + dense_up.shape, bf),
            pltpu.VMEM((ne,) + dense_down.shape, bf),
            pltpu.VMEM((ne, rows, CORES * shard), f32),
            pltpu.VMEM((ne, rows, tp * shard), bf),
            pltpu.VMEM((rows, width), f32),
            pltpu.VMEM((2, nj, half, UNIT), f32),
            pltpu.VMEM((ne, 2, nj, half, UNIT), bf),
            pltpu.VMEM((2, 2, nj, half, UNIT), bf),
            pltpu.VMEM((2, nj, half, UNIT), bf),
            pltpu.VMEM((rows, width), f32),
            pltpu.VMEM((rows, 1), f32),
            pltpu.VMEM((ne, SUB, rows), f32),
            pltpu.VMEM((ne, rows, 1), f32),
            pltpu.VMEM((topk, rows), jnp.int32),
            pltpu.VMEM((topk, rows), f32),
            pltpu.VMEM((1, width), f32),
            pltpu.VMEM((1, width), f32),
            dma((11,)),
            dma((nz, CORES, 2)),
            dma((nz,)),
            dma((nz,)),
            dma((nz,)),
            dma((2,)),
            dma((1,)),
            dma((nj, nz - 1)),
            dma((nj,)),
            dma((1,)),
            dma((4,)),
            dma((ne,)),
            dma((6,)),
            dma((2, 3)),
            dma((1,)),
            dma((nj, 2)),
        ],
        compiler_params=pltpu.CompilerParams(
            collective_id=0, has_side_effects=True, vmem_limit_bytes=VMEM_BYTES
        ),
        cost_estimate=pl.CostEstimate(
            flops=flops, bytes_accessed=8 * rows * width, transcendentals=ne * rows * shard * tp
        ),
    )(
        tokens, w_gate[0], w_up[0], w_down[0], dense_gate, dense_up, dense_down,
        expert_ids.T, gate_weights.T, norm_gain.reshape(1, width), mix_vector.reshape(1, width),
    )


def fits(ne, tp, tokens, w_gate, dense_gate):
    rows, width = tokens.shape
    shard = w_gate.shape[2]
    block = rows * width
    size = 2 * ne * block * 2 + 24 * block + 6 * width * shard * tp
    size += 2 * ne * rows * shard * tp + 6 * ne * dense_gate.size + 1024 * ne * rows
    size += 8 * ne * rows * shard
    aligned = shard % 128 == 0 and width % (8 * UNIT) == 0 and width > TAIL and rows % 64 == 0
    return ne == 4 and tp == 4 * CORES and aligned and size < VMEM_BYTES * 15 // 16


def dense_branch(normed, dense_gate, dense_up, dense_down, mix_vector):
    dense_g = jnp.dot(
        normed,
        lax.all_gather(dense_gate, "ep", axis=0, tiled=True),
        preferred_element_type=jnp.float32,
    )
    dense_u = jnp.dot(
        normed,
        lax.all_gather(dense_up, "ep", axis=0, tiled=True),
        preferred_element_type=jnp.float32,
    )
    dense_hidden = (jax.nn.silu(dense_g) * dense_u).astype(jnp.bfloat16)
    dense_out = jnp.dot(
        dense_hidden,
        lax.all_gather(dense_down, "ep", axis=1, tiled=True),
        preferred_element_type=jnp.float32,
    )
    mix = jax.nn.sigmoid(jnp.sum(normed.astype(jnp.float32) * mix_vector, axis=1))
    return mix[:, None] * dense_out


def on_device(
    tokens,
    norm_gain,
    expert_ids,
    gate_weights,
    w_gate,
    w_up,
    w_down,
    dense_gate,
    dense_up,
    dense_down,
    mix_vector,
):
    groups = lax.axis_size("ep")
    ring = lax.axis_size("tp")
    if fits(groups, ring, tokens, w_gate, dense_gate):
        return fused_layer(
            groups, ring, tokens, norm_gain, expert_ids, gate_weights,
            w_gate, w_up, w_down, dense_gate, dense_up, dense_down, mix_vector,
        )
    values = tokens.astype(jnp.float32)
    scale = lax.rsqrt(jnp.mean(values * values, axis=1, keepdims=True) + eps)
    normed = (values * scale * norm_gain).astype(jnp.bfloat16)
    count_tok, topk = expert_ids.shape
    width = tokens.shape[1]
    capacity = 2 * count_tok * topk // groups
    flat_ids = expert_ids.reshape(-1)
    onehot = (flat_ids[:, None] == jnp.arange(groups, dtype=jnp.int32)[None, :]).astype(jnp.int32)
    before = jnp.cumsum(onehot, axis=0) - onehot
    slot = jnp.sum(before * onehot, axis=1)
    dest = flat_ids * capacity + slot
    owner = jnp.arange(count_tok * topk, dtype=jnp.int32) // topk
    buffer = jnp.zeros((groups * capacity, width), jnp.bfloat16).at[dest].set(normed[owner])
    arrived = lax.all_to_all(
        buffer.reshape(groups, capacity, width), "ep", split_axis=0, concat_axis=0, tiled=True
    )
    rows = arrived.reshape(groups * capacity, width)
    gate = jnp.dot(
        rows,
        lax.all_gather(w_gate, "tp", axis=2, tiled=True)[0],
        preferred_element_type=jnp.float32,
    )
    upper = jnp.dot(
        rows, lax.all_gather(w_up, "tp", axis=2, tiled=True)[0], preferred_element_type=jnp.float32
    )
    hidden_all = (jax.nn.silu(gate) * upper).astype(jnp.bfloat16)
    expert_out = lax.dot_general(
        hidden_all,
        lax.all_gather(w_down, "tp", axis=2, tiled=True)[0],
        (((1,), (1,)), ((), ())),
        preferred_element_type=jnp.float32,
    )
    results = expert_out.astype(jnp.bfloat16).reshape(groups, capacity, width)
    returned = lax.all_to_all(results, "ep", split_axis=0, concat_axis=0, tiled=True)
    picked = returned.reshape(groups * capacity, width)[dest].reshape(count_tok, topk, width)
    routed = jnp.einsum("tk,tkd->td", gate_weights, picked.astype(jnp.float32))
    side = dense_branch(normed, dense_gate, dense_up, dense_down, mix_vector)
    return (routed + side).astype(jnp.bfloat16)


def solution(mesh):
    placed = (
        P(("ep", "tp"), None),
        P(),
        P(("ep", "tp"), None),
        P(("ep", "tp"), None),
        P("ep", None, "tp"),
        P("ep", None, "tp"),
        P("ep", None, "tp"),
        P("ep", None),
        P("ep", None),
        P(None, "ep"),
        P(),
    )
    return jax.shard_map(
        on_device, mesh=mesh, in_specs=placed, out_specs=P(("ep", "tp"), None), check_vma=False
    )
```

```python
import functools

import jax
import jax.numpy as jnp
from jax import lax
from jax.experimental import pallas as pl
from jax.experimental.pallas import tpu as pltpu
from jax.sharding import PartitionSpec as P

MESH = pl.DeviceIdType.MESH
VMEM_BYTES = 64000 * 1024
CORES = 2
UNIT = 128
LOOK = 2
BEHIND = 2
TAIL = 256
SUB = 8
eps = 1e-06


def moe_kernel(
    ne, nz, x_hbm, wg_hbm, wu_hbm, wd_hbm, dg_hbm, du_hbm, dd_hbm, ids_hbm, gates_hbm,
    gain_hbm, mixv_hbm, out_ref,
    xin, xg, ws, dgs, dus, dds, gbuf, hbuf, own, keep, ysend, yrecv, relay, side, mix_ref, wts, wcol,
    ids_ref, gates_ref, gain_ref, mixv_ref,
    lsem, wrecv, wright, wleft, wpartner, xsend, xrecv, crecv, precv,
    tsend, trecv, gsem, dsem, drecv, rsend, rrecv,
):
    me = lax.axis_index("ep")
    tp = lax.axis_index("tp")
    z = tp // CORES
    c = tp % CORES
    rows, width = xg.shape[1], xg.shape[2]
    nj = crecv.shape[0]
    half = rows // 2
    shard = ws.shape[4]
    across, along, diagonal = me + 1 - 2 * (me % 2), (me + 2) % ne, ne - 1 - me
    peers = [across, along, diagonal]
    partner = z * CORES + (1 - c)

    barrier = pltpu.get_barrier_semaphore()
    for peer in (across, along):
        pl.semaphore_signal(barrier, inc=1, device_id={"ep": peer}, device_id_type=MESH)
    pl.semaphore_signal(barrier, inc=1, device_id={"tp": partner}, device_id_type=MESH)

    @pl.when(z > 0)
    def _():
        pl.semaphore_signal(barrier, inc=1, device_id={"tp": tp - CORES}, device_id_type=MESH)

    @pl.when(z < nz - 1)
    def _():
        pl.semaphore_signal(barrier, inc=1, device_id={"tp": tp + CORES}, device_id_type=MESH)

    local = [pltpu.make_async_copy(wg_hbm, ws.at[z, c, 0], lsem.at[0])]
    local.append(pltpu.make_async_copy(wu_hbm, ws.at[z, c, 1], lsem.at[1]))
    local.append(pltpu.make_async_copy(x_hbm, xin, lsem.at[2]))
    local.append(pltpu.make_async_copy(wd_hbm, ws.at[z, c, 2], lsem.at[3]))
    for p, (ref, slot) in enumerate(((dg_hbm, dgs), (du_hbm, dus), (dd_hbm, dds))):
        local.append(pltpu.make_async_copy(ref, slot.at[0], lsem.at[4 + p]))
    smalls = ((ids_hbm, ids_ref), (gates_hbm, gates_ref), (gain_hbm, gain_ref), (mixv_hbm, mixv_ref))
    for p, (ref, slot) in enumerate(smalls):
        local.append(pltpu.make_async_copy(ref, slot, lsem.at[7 + p]))
    for copy in local:
        copy.start()

    neighbours = (z + nz - 1) // nz + (2 * nz - 2 - z) // nz
    with jax.named_scope("barrier"):
        pl.semaphore_wait(barrier, 3 + neighbours)

    def remote(src, dst, send, recv, **device):
        return pltpu.make_async_remote_copy(
            src_ref=src, dst_ref=dst, send_sem=send, recv_sem=recv,
            device_id=device, device_id_type=MESH,
        )

    def weight_copy(src, p, target, sems):
        piece = ws.at[src, c, p]
        return remote(piece, piece, sems.at[src], wrecv.at[src, c, p], tp=target)

    def to_right(src, p):
        weight_copy(src, p, tp + CORES, wright).start()

    def to_left(src, p):
        weight_copy(src, p, tp - CORES, wleft).start()

    def to_partner(src, p):
        weight_copy(src, p, partner, wpartner).start()

    def await_piece(src, color, p):
        piece = ws.at[src, color, p]
        remote(piece, piece, wpartner.at[src], wrecv.at[src, color, p], tp=partner).wait_recv()

    def await_sent(src, sems, count):
        piece = ws.at[src, c, :count]
        remote(piece, piece, sems.at[src], wrecv.at[src, c, 0], tp=partner).wait_send()

    def far_main(src, color, target):
        piece = ws.at[src, color, 1] if color else ws.at[src, 0, 1, : width - TAIL]
        return remote(piece, piece, xsend.at[0], wrecv.at[src, color, 1], tp=target)

    def far_tail(src, target):
        piece = ws.at[src, 0, 1, width - TAIL :]
        return remote(piece, piece, xsend.at[1], xrecv.at[0], tp=target)

    def by_color(fn):
        for color in range(CORES):
            pl.when(c == color)(functools.partial(fn, color))

    def at(j, fn):
        if not isinstance(j, int):
            pl.when((j >= 0) & (j < nj))(lambda: fn(j))
        elif 0 <= j < nj:
            fn(j)

    def columns(j):
        return pl.ds(pl.multiple_of(j * UNIT, UNIT), UNIT)

    def chunk_copy(src, j, target, sems, recv):
        piece = ws.at[src, c, 2, columns(j)]
        return remote(piece, piece, sems.at[src], recv, tp=target)

    def order(src, there):
        return (src - there + nz) % nz - 1

    def c_right(src, j):
        chunk_copy(src, j, tp + CORES, wright, crecv.at[j, order(src, z + 1)]).start()

    def c_left(src, j):
        chunk_copy(src, j, tp - CORES, wleft, crecv.at[j, order(src, z - 1)]).start()

    def c_partner(src, j):
        chunk_copy(src, j, partner, wpartner, precv.at[j]).start()

    def arrive(src, j):
        chunk_copy(src, j, partner, wpartner, crecv.at[j, order(src, z)]).wait_recv()
        c_partner(src, j)

    def token_copy(k):
        block = (me, me, across, along)[k]
        peer = (across, along, along, across)[k]
        low, size = ((0, rows), (0, rows), (0, half), (half, half))[k]
        piece = xg.at[block, low : low + size]
        return remote(piece, piece, tsend.at[0], trecv.at[k], ep=peer)

    def await_token(k):
        block = (across, along, diagonal, diagonal)[k]
        low, size = ((0, rows), (0, rows), (0, half), (half, half))[k]
        piece = xg.at[block, low : low + size]
        remote(piece, piece, tsend.at[0], trecv.at[k], ep=across).wait_recv()

    def gate_copy(k):
        return remote(wts.at[0], wts.at[1 + k], gsem.at[0], gsem.at[1 + k], ep=peers[k])

    def gate_all():
        piece = wts.at[1:]
        return remote(piece, piece, gsem.at[0], gsem.at[1], ep=across)

    def await_gate(k):
        piece = wts.at[1 + k]
        remote(piece, piece, gsem.at[0], gsem.at[1 + k], ep=across).wait_recv()

    def dense_piece(p, blocks, color):
        slot = (dgs, dus, dds)[p]
        part = slot.shape[1] // CORES
        return slot.at[blocks, pl.ds(pl.multiple_of(color * part, part), part)]

    def dense_copy(k, p):
        lands = dense_piece(p, 1 + k, c)
        return remote(dense_piece(p, 0, c), lands, dsem.at[p], drecv.at[0, p], ep=peers[k])

    def dense_partner(k, p):
        piece = dense_piece(p, 1 + k, c)
        return remote(piece, piece, dsem.at[3 + p], drecv.at[1, p], tp=partner)

    def dense_all(p, i, color):
        piece = dense_piece(p, pl.ds(1, ne - 1), color)
        return remote(piece, piece, dsem.at[3 * i + p], drecv.at[i, p], tp=partner)

    for p in range(2):
        local[p].wait()

        @pl.when(z < nz - 1)
        def _():
            to_right(z, p)

        @pl.when(z > 0)
        def _():
            to_left(z, p)

        to_partner(z, p)
    for p in (2, 7, 8, 9, 10):
        local[p].wait()

    expert = lax.broadcasted_iota(jnp.int32, (SUB, rows), 0)
    named, gate = ids_ref[...], gates_ref[...]
    weight = jnp.zeros((SUB, rows), jnp.float32)
    for k in range(ids_ref.shape[0]):
        weight += jnp.where(named[k : k + 1, :] == expert, gate[k : k + 1, :], 0.0)
    wts[0] = weight
    tile = 32

    def norm(i, carry):
        at = pl.ds(pl.multiple_of(i * tile, tile), tile)
        v = xin[at, :].astype(jnp.float32)
        scale = lax.rsqrt(jnp.sum(v * v, axis=1, keepdims=True) * (1.0 / width) + eps)
        n = (v * scale * gain_ref[...]).astype(jnp.bfloat16)
        xg[me, at, :] = n
        m = jnp.sum(n.astype(jnp.float32) * mixv_ref[...], axis=1, keepdims=True)
        mix_ref[at, :] = 1.0 / (1.0 + jnp.exp(-m))
        return carry

    with jax.named_scope("norm"):
        lax.fori_loop(0, rows // tile, norm, 0)
    local[3].wait()

    def own_chunks(j, carry):
        c_partner(z, j)

        @pl.when(z == 0)
        def _():
            c_right(z, j)

        @pl.when(z == nz - 1)
        def _():
            c_left(z, j)

        return carry

    lax.fori_loop(0, nj, own_chunks, 0)
    for k in range(2):
        token_copy(k).start()
    for k in range(2):
        gate_copy(k).start()

    def forward(d, p):
        @pl.when(z >= d)
        def _():
            await_piece(z - d, c, p)

            @pl.when(z < nz - 1)
            def _():
                if d == nz - 2 and p == 1:
                    by_color(lambda color: far_main(z - d, color, tp + CORES).start())
                else:
                    to_right(z - d, p)

            to_partner(z - d, p)

        @pl.when(z + d < nz)
        def _():
            await_piece(z + d, c, p)

            @pl.when(z > 0)
            def _():
                if d == nz - 2 and p == 1:
                    by_color(lambda color: far_main(z + d, color, tp - CORES).start())
                else:
                    to_left(z + d, p)

            to_partner(z + d, p)

    def weight_of(src, p):
        return jnp.concatenate([ws[src, i, p] for i in range(CORES)], axis=1)

    def gate_part(src):
        await_piece(src, 1 - c, 0)

        def one(b, carry):
            g = jnp.dot(xg[b], weight_of(src, 0), preferred_element_type=jnp.float32)
            gbuf[b] = g / (1.0 + jnp.exp(-g)) * wcol[b]
            return carry

        lax.fori_loop(0, ne, one, 0)

    def far_forward():
        src = nz - 1 - z

        def one(color):
            far_main(src, color, partner).wait_recv()
            far_main(src, color, partner).start()
            if color:
                far_tail(src, partner).wait_recv()
                far_tail(src, partner).start()

        by_color(one)

    def far_await(src):
        def one(color):
            far_main(src, 1 - color, partner).wait_recv()
            if not color:
                far_tail(src, partner).wait_recv()

        by_color(one)

    def up_part(src, far=False):
        if far:
            far_await(src)
        else:
            await_piece(src, 1 - c, 1)

            @pl.when((c == 1) & (z == 1) & (src == nz - 1))
            def _():
                far_tail(src, tp - CORES).start()

            @pl.when((c == 1) & (z == nz - 2) & (src == 0))
            def _():
                far_tail(src, tp + CORES).start()

        here = pl.ds(pl.multiple_of(src * (CORES * shard), CORES * shard), CORES * shard)

        def one(b, carry):
            u = jnp.dot(xg[b], weight_of(src, 1), preferred_element_type=jnp.float32)
            hbuf[b, :, here] = (gbuf[b] * u).astype(jnp.bfloat16)
            return carry

        lax.fori_loop(0, ne, one, 0)

    def hidden(src):
        gate_part(src)
        up_part(src)

    def both(d, fn):
        @pl.when(z >= d)
        def _():
            fn(z - d)

        @pl.when(z + d < nz)
        def _():
            fn(z + d)

    def ahead(t):
        def one(d, j):
            @pl.when(z == 1)
            def _():
                if d == 0:
                    c_right(z, j)
                elif d == 1:
                    arrive(z - 1, j)
                    c_right(z - 1, j)
                    arrive(z + 1, j)
                else:
                    arrive(z + 2, j)
                    for src in range(nz - 1):
                        c_left(z + src, j)

            @pl.when(z == 2)
            def _():
                if d == 0:
                    c_left(z, j)
                elif d == 1:
                    arrive(z + 1, j)
                    c_left(z + 1, j)
                    arrive(z - 1, j)
                else:
                    arrive(z - 2, j)
                    for src in range(nz - 1):
                        c_right(z - src, j)

        for d in range(nz - 1):
            at(t + LOOK * (nz - 1 - d), functools.partial(one, d))

    for p in range(2):
        with jax.named_scope(f"forward1_{p}"):
            forward(1, p)
    with jax.named_scope("token_relay"):
        for k in range(2):
            await_token(k)
            token_copy(2 + k).start()
    gate_copy(2).start()
    for p in range(3):
        local[4 + p].wait()
        for k in range(ne - 1):
            dense_copy(k, p).start()
    for d in range(2, nz - 1):
        for p in range(2):
            with jax.named_scope(f"forward{d}_{p}"):
                forward(d, p)
    for t in range(LOOK):
        ahead(t - LOOK * (nz - 1))
    with jax.named_scope("gate_wait"):
        for k in range(ne - 1):
            await_gate(k)
    lane = lax.broadcasted_iota(jnp.int32, (rows, SUB), 1)
    for r, b in enumerate([me] + peers):
        column = jnp.where(lane == me, wts[r].T, 0.0)
        wcol[b] = jnp.sum(column, axis=1, keepdims=True)
    with jax.named_scope("token_wait"):
        for k in range(2, 4):
            await_token(k)
    with jax.named_scope("hidden_own"):
        hidden(z)
    for d in range(1, nz - 1):
        with jax.named_scope(f"hidden{d}"):
            both(d, hidden)
        with jax.named_scope(f"ahead{d}"):
            for t in range(LOOK):
                ahead(t - LOOK * (nz - 1 - d))
    with jax.named_scope("dense_wait"):
        for p in range(3):
            dense_all(p, 0, c).wait_recv()
            for k in range(ne - 1):
                dense_partner(k, p).start()
    with jax.named_scope("forward_last0"):
        forward(nz - 1, 0)
    with jax.named_scope("gate_last"):
        both(nz - 1, gate_part)
    with jax.named_scope("dense_partner"):
        for p in range(3):
            dense_all(p, 1, 1 - c).wait_recv()
    with jax.named_scope("dense_side"):
        dense_side([me] + peers, me, xg, dgs, dus, dds, mix_ref, side)
    with jax.named_scope("forward_last1"):
        pl.when((z == 0) | (z == nz - 1))(far_forward)
    with jax.named_scope("up_last"):
        both(nz - 1, functools.partial(up_part, far=True))

    def back(k, j):
        block = (diagonal, diagonal, across, along, along, across)[k]
        peer = (across, along, across, along, along, across)[k]
        spot = (0, 1, 0, 1, 1, 0)[k]
        lands = relay.at[k, j] if k < 2 else yrecv.at[spot, k % 2, j]
        return remote(ysend.at[block, k % 2, j], lands, rsend.at[0], rrecv.at[j, min(k // 2, 1)], ep=peer)

    def take(j):
        ahead(j)

        @pl.when(z == 0)
        def _():
            for d in range(1, nz):
                arrive(d, j)

        @pl.when(z == nz - 1)
        def _():
            for d in range(1, nz):
                arrive(z - d, j)

        piece = ws.at[:, 1 - c, 2, columns(j)]
        remote(piece, piece, wpartner.at[0], precv.at[j], tp=partner).wait_recv()

    def produce(j):
        here = columns(j)
        w = jnp.concatenate([ws[s, i, 2, here, :] for s in range(nz) for i in range(CORES)], axis=1)
        blocks = (diagonal, across, along, me)
        full = lax.dot_general(
            jnp.concatenate([hbuf[b] for b in blocks], axis=0), w,
            (((1,), (1,)), ((), ())), preferred_element_type=jnp.float32,
        )
        y = [full[i * half : (i + 1) * half] for i in range(2 * ne)]
        for k, i in enumerate((0, 1, 2, 5)):
            ysend[blocks[i // 2], i % 2, j] = y[i].astype(jnp.bfloat16)
            back(k, j).start()
        keep[0, j] = y[4]
        keep[1, j] = y[3]
        own[:, here] = full[(ne - 1) * rows :]

    def pass_on(j):
        piece = relay.at[:, j]
        remote(piece, piece, rsend.at[0], rrecv.at[j, 0], ep=across).wait_recv()
        for k, block in enumerate((along, across)):
            v = keep[k, j] + relay[k, j].astype(jnp.float32)
            ysend[block, k, j] = v.astype(jnp.bfloat16)
            back(4 + k, j).start()

    def combine(j):
        piece = yrecv.at[:, :, j]
        remote(piece, piece, rsend.at[0], rrecv.at[j, 1], ep=across).wait_recv()
        here = columns(j)
        for h in range(2):
            low = h * half
            total = side[low : low + half, here] + own[low : low + half, here]
            for k in range(2):
                total = total + yrecv[k, h, j].astype(jnp.float32)
            out_ref[low : low + half, here] = total.astype(jnp.bfloat16)

    def step(j, carry):
        with jax.named_scope("take"):
            take(j)
        with jax.named_scope("pass_on"):
            pl.when(j < nj - 1)(lambda: at(j - BEHIND, pass_on))
        with jax.named_scope("produce"):
            produce(j)
        with jax.named_scope("combine"):
            pl.when(j < nj - 2)(lambda: at(j - 2 * BEHIND, combine))
        return carry

    lax.fori_loop(0, nj, step, 0)

    def pass_rest(j, carry):
        pass_on(j)
        return carry

    def combine_rest(j, carry):
        combine(j)
        return carry

    with jax.named_scope("pass_rest"):
        lax.fori_loop(nj - 1 - BEHIND, nj, pass_rest, 0)
    with jax.named_scope("combine_rest"):
        lax.fori_loop(nj - 2 * BEHIND - 2, nj, combine_rest, 0)

    drain = jax.named_scope("drain")
    drain.__enter__()
    piece = xg.at[: ne - 1]
    remote(piece, piece, tsend.at[0], trecv.at[0], ep=across).wait_send()
    gate_all().wait_send()
    for p in range(3):
        for i in range(2):
            dense_all(p, i, c).wait_send()
    for src in range(nz):
        for sems, there, far in (
            (wright, (z < nz - 1) & (z >= src), (z == nz - 2) & (src == 0)),
            (wleft, (z > 0) & (z <= src), (z == 1) & (src == nz - 1)),
            (wpartner, z >= 0, (z == nz - 1 - src) & (src % (nz - 1) == 0)),
        ):
            pl.when(there & far)(functools.partial(await_sent, src, sems, 2))
            pl.when(there & jnp.logical_not(far))(functools.partial(await_sent, src, sems, 3))

    def far_sent(color):
        far_main(0, color, partner).wait_send()
        if color:
            far_tail(0, partner).wait_send()

    by_color(far_sent)
    piece = ysend.at[: ne - 1]
    remote(piece, piece, rsend.at[0], rrecv.at[0, 0], ep=across).wait_send()
    drain.__exit__(None, None, None)


def dense_side(owners, me, xg, dgs, dus, dds, mix_ref, side):
    deep, wide = dgs.shape[1], dds.shape[2]
    g = u = None
    for r, e in enumerate(owners):
        x = xg[me, :, pl.ds(pl.multiple_of(e * deep, deep), deep)]
        ge = jnp.dot(x, dgs[r], preferred_element_type=jnp.float32)
        ue = jnp.dot(x, dus[r], preferred_element_type=jnp.float32)
        g, u = (ge, ue) if r == 0 else (g + ge, u + ue)
    h = (g / (1.0 + jnp.exp(-g)) * u).astype(jnp.bfloat16)
    for r, e in enumerate(owners):
        o = jnp.dot(h, dds[r], preferred_element_type=jnp.float32)
        side[:, pl.ds(pl.multiple_of(e * wide, wide), wide)] = mix_ref[...] * o


def fused_layer(
    ne, tp, tokens, norm_gain, expert_ids, gate_weights,
    w_gate, w_up, w_down, dense_gate, dense_up, dense_down, mix_vector,
):
    nz = tp // CORES
    rows, width = tokens.shape
    topk = expert_ids.shape[1]
    shard = w_gate.shape[2]
    nj = width // UNIT
    half = rows // 2
    bf, f32 = jnp.bfloat16, jnp.float32
    dma = pltpu.SemaphoreType.DMA
    hbm = pl.BlockSpec(memory_space=pl.ANY)
    vmem = pl.BlockSpec(memory_space=pltpu.VMEM)
    flops = 6 * ne * rows * width * shard * tp
    return pl.pallas_call(
        functools.partial(moe_kernel, ne, nz),
        out_shape=pltpu.VMEM((rows, width), bf),
        in_specs=[hbm] * 11,
        out_specs=vmem,
        scratch_shapes=[
            pltpu.VMEM((rows, width), bf),
            pltpu.VMEM((ne, rows, width), bf),
            pltpu.VMEM((nz, CORES, 3, width, shard), bf),
            pltpu.VMEM((ne,) + dense_gate.shape, bf),
            pltpu.VMEM((ne,) + dense_up.shape, bf),
            pltpu.VMEM((ne,) + dense_down.shape, bf),
            pltpu.VMEM((ne, rows, CORES * shard), f32),
            pltpu.VMEM((ne, rows, tp * shard), bf),
            pltpu.VMEM((rows, width), f32),
            pltpu.VMEM((2, nj, half, UNIT), f32),
            pltpu.VMEM((ne, 2, nj, half, UNIT), bf),
            pltpu.VMEM((2, 2, nj, half, UNIT), bf),
            pltpu.VMEM((2, nj, half, UNIT), bf),
            pltpu.VMEM((rows, width), f32),
            pltpu.VMEM((rows, 1), f32),
            pltpu.VMEM((ne, SUB, rows), f32),
            pltpu.VMEM((ne, rows, 1), f32),
            pltpu.VMEM((topk, rows), jnp.int32),
            pltpu.VMEM((topk, rows), f32),
            pltpu.VMEM((1, width), f32),
            pltpu.VMEM((1, width), f32),
            dma((11,)),
            dma((nz, CORES, 2)),
            dma((nz,)),
            dma((nz,)),
            dma((nz,)),
            dma((2,)),
            dma((1,)),
            dma((nj, nz - 1)),
            dma((nj,)),
            dma((1,)),
            dma((4,)),
            dma((ne,)),
            dma((6,)),
            dma((2, 3)),
            dma((1,)),
            dma((nj, 2)),
        ],
        compiler_params=pltpu.CompilerParams(
            collective_id=0, has_side_effects=True, vmem_limit_bytes=VMEM_BYTES
        ),
        cost_estimate=pl.CostEstimate(
            flops=flops, bytes_accessed=8 * rows * width, transcendentals=ne * rows * shard * tp
        ),
    )(
        tokens, w_gate[0], w_up[0], w_down[0], dense_gate, dense_up, dense_down,
        expert_ids.T, gate_weights.T, norm_gain.reshape(1, width), mix_vector.reshape(1, width),
    )


def fits(ne, tp, tokens, w_gate, dense_gate):
    rows, width = tokens.shape
    shard = w_gate.shape[2]
    block = rows * width
    size = 2 * ne * block * 2 + 24 * block + 6 * width * shard * tp
    size += 2 * ne * rows * shard * tp + 6 * ne * dense_gate.size + 1024 * ne * rows
    size += 8 * ne * rows * shard
    aligned = shard % 128 == 0 and width % (8 * UNIT) == 0 and width > TAIL and rows % 64 == 0
    return ne == 4 and tp == 4 * CORES and aligned and size < VMEM_BYTES * 15 // 16


def dense_branch(normed, dense_gate, dense_up, dense_down, mix_vector):
    dense_g = jnp.dot(
        normed,
        lax.all_gather(dense_gate, "ep", axis=0, tiled=True),
        preferred_element_type=jnp.float32,
    )
    dense_u = jnp.dot(
        normed,
        lax.all_gather(dense_up, "ep", axis=0, tiled=True),
        preferred_element_type=jnp.float32,
    )
    dense_hidden = (jax.nn.silu(dense_g) * dense_u).astype(jnp.bfloat16)
    dense_out = jnp.dot(
        dense_hidden,
        lax.all_gather(dense_down, "ep", axis=1, tiled=True),
        preferred_element_type=jnp.float32,
    )
    mix = jax.nn.sigmoid(jnp.sum(normed.astype(jnp.float32) * mix_vector, axis=1))
    return mix[:, None] * dense_out


def on_device(
    tokens,
    norm_gain,
    expert_ids,
    gate_weights,
    w_gate,
    w_up,
    w_down,
    dense_gate,
    dense_up,
    dense_down,
    mix_vector,
):
    groups = lax.axis_size("ep")
    ring = lax.axis_size("tp")
    if fits(groups, ring, tokens, w_gate, dense_gate):
        return fused_layer(
            groups, ring, tokens, norm_gain, expert_ids, gate_weights,
            w_gate, w_up, w_down, dense_gate, dense_up, dense_down, mix_vector,
        )
    values = tokens.astype(jnp.float32)
    scale = lax.rsqrt(jnp.mean(values * values, axis=1, keepdims=True) + eps)
    normed = (values * scale * norm_gain).astype(jnp.bfloat16)
    count_tok, topk = expert_ids.shape
    width = tokens.shape[1]
    capacity = 2 * count_tok * topk // groups
    flat_ids = expert_ids.reshape(-1)
    onehot = (flat_ids[:, None] == jnp.arange(groups, dtype=jnp.int32)[None, :]).astype(jnp.int32)
    before = jnp.cumsum(onehot, axis=0) - onehot
    slot = jnp.sum(before * onehot, axis=1)
    dest = flat_ids * capacity + slot
    owner = jnp.arange(count_tok * topk, dtype=jnp.int32) // topk
    buffer = jnp.zeros((groups * capacity, width), jnp.bfloat16).at[dest].set(normed[owner])
    arrived = lax.all_to_all(
        buffer.reshape(groups, capacity, width), "ep", split_axis=0, concat_axis=0, tiled=True
    )
    rows = arrived.reshape(groups * capacity, width)
    gate = jnp.dot(
        rows,
        lax.all_gather(w_gate, "tp", axis=2, tiled=True)[0],
        preferred_element_type=jnp.float32,
    )
    upper = jnp.dot(
        rows, lax.all_gather(w_up, "tp", axis=2, tiled=True)[0], preferred_element_type=jnp.float32
    )
    hidden_all = (jax.nn.silu(gate) * upper).astype(jnp.bfloat16)
    expert_out = lax.dot_general(
        hidden_all,
        lax.all_gather(w_down, "tp", axis=2, tiled=True)[0],
        (((1,), (1,)), ((), ())),
        preferred_element_type=jnp.float32,
    )
    results = expert_out.astype(jnp.bfloat16).reshape(groups, capacity, width)
    returned = lax.all_to_all(results, "ep", split_axis=0, concat_axis=0, tiled=True)
    picked = returned.reshape(groups * capacity, width)[dest].reshape(count_tok, topk, width)
    routed = jnp.einsum("tk,tkd->td", gate_weights, picked.astype(jnp.float32))
    side = dense_branch(normed, dense_gate, dense_up, dense_down, mix_vector)
    return (routed + side).astype(jnp.bfloat16)


def solution(mesh):
    placed = (
        P(("ep", "tp"), None),
        P(),
        P(("ep", "tp"), None),
        P(("ep", "tp"), None),
        P("ep", None, "tp"),
        P("ep", None, "tp"),
        P("ep", None, "tp"),
        P("ep", None),
        P("ep", None),
        P(None, "ep"),
        P(),
    )
    return jax.shard_map(
        on_device, mesh=mesh, in_specs=placed, out_specs=P(("ep", "tp"), None), check_vma=False
    )
```
